256 devices in a mesh: ep: 64 (over z, x, core), tp: 4 (over y).
Axes of the slice: x: 4, y: 4, z: 8, core: 2. Of those that a mesh axis runs over, the one named last changes fastest.
Arguments:
- tokens: bfloat16 [2048, 2048], P('ep'), may hold values from -6 to 6
- norm_gain_attn: float32 [2048], replicated, may hold values from 0.1 to 1.9
- w_query: bfloat16 [2048, 2048], P('ep', 'tp'), may hold values from -0.125 to 0.125
- w_key: bfloat16 [2048, 256], P('ep', 'tp'), may hold values from -0.125 to 0.125
- w_value: bfloat16 [2048, 256], P('ep', 'tp'), may hold values from -0.125 to 0.125
- w_forget: bfloat16 [2048, 32], P(None, 'tp'), may hold values from -0.125 to 0.125
- forget_bias: float32 [32], P('tp'), may hold values from -1 to 3
- cache_keys: bfloat16 [2048, 256, 1024], P('ep', 'tp'), may hold values from -64 to 64
- cache_values: bfloat16 [2048, 256, 1024], P('ep', 'tp'), may hold values from -6 to 6
- cache_logcum: float32 [2048, 32, 1024], P('ep', 'tp'), may hold values from -2048 to 0, as said below
- lengths: int32 [2048], P('ep'), may hold values from 1 to 1023, as said below
- w_out: bfloat16 [2048, 2048], P('tp'), may hold values from -0.125 to 0.125
- norm_gain_mix: float32 [2048], replicated, may hold values from 0.1 to 1.9
- norm_gain_ffn: float32 [2048], replicated, may hold values from 0.1 to 1.9
- expert_gate: bfloat16 [2048, 65536], P(None, ('ep', 'tp')), may hold values from -0.125 to 0.125
- expert_up: bfloat16 [2048, 65536], P(None, ('ep', 'tp')), may hold values from -0.125 to 0.125
- expert_down: bfloat16 [65536, 2048], P(('ep', 'tp')), may hold values from -0.09375 to 0.09375
- routes: int32 [2048, 2], P('ep'), may hold values from 0 to 15, all different within a row; in each aligned block of 32 rows (0 to 31, 32 to 63, ...) at most 8 rows name the same one
- route_weights: float32 [2048, 2], P('ep'), may hold values from 0.2 to 1
Outputs:
- layer_out: bfloat16 [2048, 2048], P('ep', 'tp')
- new_keys: bfloat16 [2048, 256], P('ep', 'tp')
- new_values: bfloat16 [2048, 256], P('ep', 'tp')
- new_log_gate: float32 [2048, 32], P('ep', 'tp')
The draws below stay inside these ranges and needn't reach their ends.
Inputs may be any that keep to these rules, and one draw needn't show every extreme that they name: `routes`: each row names 2 different experts. Within the rows of one index of ep no expert is named by more than 8 rows, and in every draw some expert is named by exactly 8 rows of some index. `lengths`: some sequence has 1023 cached positions in every draw. `cache_logcum`: never rising along positions (the last dimension).
All inputs are finite; a program needn't handle non-finite values.
Results may differ from the reference program's by a relative error of at most 0.013.
Values may be sent and summed in bfloat16 or wider, within the bound.
No kernel may reach another device: no remote copies, remote signals or barrier semaphores. Data moves between devices by JAX's collectives and lax.ppermute only.
A program may use at most 64 MiB of HBM per device.

```python
import math
import jax
import jax.numpy as jnp
import numpy as np
from jax import lax

D = 2048
HEAD_TOTAL = 32
KV_HEADS = 4
HEAD_DIM = 64
FF = 4096
TOP = 2
B_DEV = 32
LENGTH_LIMIT = 1024
SEQUENCE_TOTAL = 2048
EXPERTS = 16
CAP = 8
N_TP = 4


def draw_cache_logcum(key, part):
    gathered_keys = jax.random.split(key, 5)
    fast_share = 0.5
    fast_heads = jax.random.uniform(gathered_keys[0], (HEAD_TOTAL,)) < fast_share
    head_rate = jnp.where(fast_heads, 0.1, 0.5 / LENGTH_LIMIT)
    seq_factor = jnp.exp(jax.random.uniform(gathered_keys[1], (SEQUENCE_TOTAL, 1, 1), minval=-0.7, maxval=0.7))
    rough_factor = jnp.exp(jax.random.uniform(gathered_keys[2], (SEQUENCE_TOTAL, LENGTH_LIMIT, HEAD_TOTAL), minval=-0.7, maxval=0.7))
    decode_step_gates = -head_rate[None, None, :] * seq_factor * rough_factor
    spike_positions = jax.random.uniform(gathered_keys[3], (SEQUENCE_TOTAL, LENGTH_LIMIT, 1)) < 2.0 / LENGTH_LIMIT
    spike_penalty = jax.random.uniform(gathered_keys[4], (SEQUENCE_TOTAL, LENGTH_LIMIT, HEAD_TOTAL), minval=0.22, maxval=0.69)
    decode_step_gates = decode_step_gates - jnp.where(spike_positions, spike_penalty, 0.0)
    summed = jnp.cumsum(decode_step_gates, axis=1)
    return jnp.transpose(summed, (0, 2, 1)).astype(jnp.float32)


def draw_cache_keys(key, part):
    gathered_keys = jax.random.split(key, 1)
    shape_full = (SEQUENCE_TOTAL, LENGTH_LIMIT, KV_HEADS * HEAD_DIM)
    result = jnp.clip(jax.random.normal(gathered_keys[0], shape_full), -6.0, 6.0)
    return jnp.transpose(result, (0, 2, 1)).astype(jnp.bfloat16)


def draw_lengths(key, part):
    gathered_keys = jax.random.split(key, 3)
    block_tops = jax.random.randint(gathered_keys[0], (SEQUENCE_TOTAL // B_DEV, 1), LENGTH_LIMIT // 8, LENGTH_LIMIT)
    raw_draws = jax.random.randint(gathered_keys[1], (SEQUENCE_TOTAL // B_DEV, B_DEV), 0, LENGTH_LIMIT)
    seq_lengths = (1 + raw_draws % block_tops).reshape(-1)
    chosen = jax.random.randint(gathered_keys[2], (), 0, SEQUENCE_TOTAL)
    seq_lengths = seq_lengths.at[chosen].set(LENGTH_LIMIT - 1)
    return seq_lengths.astype(jnp.int32)


def block_levels(rng, dims, pieces, least, largest):
    def one(dim, shards_of):
        draws = jax.random.uniform(jax.random.fold_in(jax.random.fold_in(rng, 6), dim), (shards_of,), jnp.float32, least / len(pieces), largest / len(pieces))
        return jnp.repeat(jnp.exp(draws), dims[dim] // shards_of).reshape((-1,) + (1,) * (len(dims) - dim - 1))

    loudness = one(*pieces[0])
    for cut in pieces[1:]:
        loudness = loudness * one(*cut)
    return loudness


def assign_block(rng, own, number, rows, number_of, top, bound, lean):
    ranking = jax.random.permutation(rng, number_of)
    heavy_load, common = shares(number_of, rows * top, bound, lean, True), shares(number_of, rows * top, bound, lean, False)
    places = jnp.arange(number_of)

    def named(sizes, rotation):
        used = int((sizes > 0).sum())
        fixed = max(1, used // 4)
        passed = fixed + (places - fixed + rotation * (used - fixed)) % max(1, number_of - fixed)
        return jnp.zeros((number_of,), jnp.int32).at[ranking[jnp.where(places < fixed, places, passed)]].set(jnp.asarray(sizes, jnp.int32))

    sizes = jnp.where(number % 4 == 0, named(heavy_load, number // 4), named(common, number - number // 4 - 1))
    mixed = jax.random.permutation(jax.random.fold_in(own, 3), number_of)
    donor, receiver = mixed[0:number_of // 2 * 2:2], mixed[1:number_of // 2 * 2:2]
    margin = jnp.minimum(sizes[donor] - 1, bound - sizes[receiver]) // 2
    margin = jnp.where((donor == ranking[0]) | (receiver == ranking[0]) | (sizes[receiver] == 0), 0, jnp.maximum(margin, 0))
    passed = jax.random.randint(jax.random.fold_in(own, 4), (number_of // 2,), 0, 1 << 20) % (margin + 1)
    sizes = sizes.at[donor].add(-passed).at[receiver].add(passed)
    labels = jnp.searchsorted(jnp.cumsum(sizes), jnp.arange(rows * top), side="right").astype(jnp.int32)
    grid = labels.reshape(top, rows).T
    grid = grid[jax.random.permutation(jax.random.fold_in(own, 1), rows)]
    rotation = jax.random.randint(jax.random.fold_in(own, 2), (rows, 1), 0, top)
    return jnp.take_along_axis(grid, (jnp.arange(top)[None, :] + rotation) % top, axis=1)


def shares(count, total, bound, lean, full):
    loads = [(1 << 20) // math.isqrt(rank ** lean) + 1 for rank in range(1, count + 1)]
    largest = bound if full else min(bound, max(-(-total // count), total * loads[0] // sum(loads)))
    least = 1 if total - largest >= count - 1 else 0
    holding, rest = [largest] + [least] * (count - 1), total - largest - least * (count - 1)
    while rest > 0:
        candidates = [i for i in range(1, count) if holding[i] < largest] or [i for i in range(1, count) if holding[i] < bound]
        pool, remaining = sum([loads[i] for i in candidates]), rest
        for i in candidates:
            addition = min(bound - holding[i], max(1, remaining * loads[i] // pool), rest)
            holding[i] = holding[i] + addition
            rest = rest - addition
    return np.array(holding)


def bell_draw(rng, shape, width, most, cuts=(), kind=jnp.bfloat16):
    level = block_levels(rng, shape, cuts, -0.22, 0.18) if cuts else 1.0
    values = jax.random.normal(rng, shape, jnp.float32) * width * level
    return jnp.minimum(jnp.maximum(values, -most), most).astype(kind)


def setup_inputs(seed: int = 0) -> dict:
    streams_of = jax.random.split(jax.random.key(seed), 20)
    tokens = bell_draw(streams_of[0], (SEQUENCE_TOTAL, D), 1.0, 6.0, ((0, 64),))
    norm_gain_attn = jnp.clip(1.0 + 0.18 * jax.random.normal(streams_of[1], (D,), jnp.float32), 0.1, 1.9)
    w_query = bell_draw(streams_of[2], (D, HEAD_TOTAL * HEAD_DIM), D ** -0.5, 0.125, ((0, 64), (1, 4)))
    w_key = bell_draw(streams_of[3], (D, KV_HEADS * HEAD_DIM), D ** -0.5, 0.125, ((0, 64), (1, 4)))
    w_value = bell_draw(streams_of[4], (D, KV_HEADS * HEAD_DIM), D ** -0.5, 0.125, ((0, 64), (1, 4)))
    w_forget = bell_draw(streams_of[5], (D, HEAD_TOTAL), D ** -0.5, 0.125, ((1, 4),))
    forget_bias = jnp.clip(-1.0 + 4.0 * jax.random.uniform(streams_of[6], (HEAD_TOTAL,), jnp.float32) ** block_levels(streams_of[6], (HEAD_TOTAL,), ((0, 4),), -0.2, 0.2), -1.0, 3.0)
    cache_keys = draw_cache_keys(jax.random.fold_in(streams_of[19], 71), 0)
    cache_values = bell_draw(streams_of[8], (SEQUENCE_TOTAL, KV_HEADS * HEAD_DIM, LENGTH_LIMIT), 1.0, 6.0, ((0, 64), (1, 4)))
    cache_logcum = draw_cache_logcum(jax.random.fold_in(streams_of[19], 71), 0)
    lengths = draw_lengths(jax.random.fold_in(streams_of[19], 71), 0)
    w_out = bell_draw(streams_of[11], (HEAD_TOTAL * HEAD_DIM, D), (HEAD_TOTAL * HEAD_DIM) ** -0.5, 0.125, ((0, 4),))
    norm_gain_mix = jnp.clip(1.0 + 0.18 * jax.random.normal(streams_of[12], (D,), jnp.float32), 0.1, 1.9)
    norm_gain_ffn = jnp.clip(1.0 + 0.18 * jax.random.normal(streams_of[13], (D,), jnp.float32), 0.1, 1.9)
    expert_gate = bell_draw(streams_of[14], (D, EXPERTS * FF), D ** -0.5, 0.125, ((1, 256),))
    expert_up = bell_draw(streams_of[15], (D, EXPERTS * FF), D ** -0.5, 0.125, ((1, 256),))
    expert_down = bell_draw(streams_of[16], (EXPERTS * FF, D), FF ** -0.5, 0.09375, ((0, 256),))
    routes_keys = jax.random.split(jax.random.fold_in(streams_of[17], 1), SEQUENCE_TOTAL // B_DEV)
    routes_turns = jax.random.permutation(jax.random.fold_in(streams_of[17], 3), SEQUENCE_TOTAL // B_DEV)
    routes = jax.vmap(lambda own, number: assign_block(jax.random.fold_in(streams_of[17], 2), own, number, B_DEV, EXPERTS, TOP, CAP, 2))(routes_keys, routes_turns).reshape((SEQUENCE_TOTAL, TOP))
    route_weights = jnp.clip(jnp.exp(math.log(1.0) - 1.609438 * jax.random.uniform(streams_of[18], (SEQUENCE_TOTAL, TOP), jnp.float32) ** block_levels(streams_of[18], (SEQUENCE_TOTAL, TOP), ((0, 64),), -0.2, 0.2)), 0.2, 1.0)
    return dict(tokens=tokens, norm_gain_attn=norm_gain_attn, w_query=w_query, w_key=w_key, w_value=w_value, w_forget=w_forget, forget_bias=forget_bias, cache_keys=cache_keys, cache_values=cache_values, cache_logcum=cache_logcum, lengths=lengths, w_out=w_out, norm_gain_mix=norm_gain_mix, norm_gain_ffn=norm_gain_ffn, expert_gate=expert_gate, expert_up=expert_up, expert_down=expert_down, routes=routes, route_weights=route_weights)


EPSILON = 1e-06
MASKED = -1e+30

def rms_scaled(field, gain_vector):
    return field * lax.rsqrt(lax.optimization_barrier(jnp.mean(field * field, axis=-1, keepdims=True)) + EPSILON) * gain_vector

def attend(query, new_key, new_value, log_gate, key_cache, value_cache, logcum, seq_lengths):
    count = query.shape[0]
    scale = HEAD_DIM ** (-0.5)
    group = HEAD_TOTAL // KV_HEADS
    query_heads = query.astype(jnp.float32).reshape(count, KV_HEADS, group, HEAD_DIM)
    key_heads = key_cache.astype(jnp.float32).reshape(count, KV_HEADS, HEAD_DIM, LENGTH_LIMIT)
    value_heads = value_cache.astype(jnp.float32).reshape(count, KV_HEADS, HEAD_DIM, LENGTH_LIMIT)
    scores = jnp.einsum('bkgd,bkdl->bkgl', query_heads, key_heads).reshape(count, HEAD_TOTAL, LENGTH_LIMIT) * scale
    own_key = new_key.astype(jnp.float32).reshape(count, KV_HEADS, 1, HEAD_DIM)
    own_score = lax.optimization_barrier(jnp.sum(query_heads * own_key, axis=-1)).reshape(count, HEAD_TOTAL) * scale
    index = jnp.broadcast_to((seq_lengths - 1).astype(jnp.int32)[:, None, None], (count, HEAD_TOTAL, 1))
    last_cum = jnp.take_along_axis(logcum, index, axis=2)[:, :, 0]
    shift = (last_cum + log_gate)[:, :, None] - logcum
    places = jnp.arange(LENGTH_LIMIT, dtype=jnp.int32)
    valid = (places[None, :] < seq_lengths[:, None])[:, None, :]
    past = jnp.where(valid, scores + shift, MASKED)
    peak = jnp.maximum(lax.optimization_barrier(jnp.max(past, axis=-1)), own_score)
    past_exp = jnp.exp(past - peak[:, :, None])
    own_exp = jnp.exp(own_score - peak)
    total = lax.optimization_barrier(jnp.sum(past_exp, axis=-1)) + own_exp
    past_weight = lax.optimization_barrier((past_exp / total[:, :, None]).astype(jnp.bfloat16)).astype(jnp.float32)
    own_weight = lax.optimization_barrier((own_exp / total).astype(jnp.bfloat16)).astype(jnp.float32)
    past_weight = past_weight.reshape(count, KV_HEADS, group, LENGTH_LIMIT)
    mixed = jnp.einsum('bkgl,bkdl->bkgd', past_weight, value_heads)
    own_value = new_value.astype(jnp.float32).reshape(count, KV_HEADS, 1, HEAD_DIM)
    mixed = mixed + own_weight.reshape(count, KV_HEADS, group)[:, :, :, None] * own_value
    return mixed.astype(jnp.bfloat16).reshape(count, HEAD_TOTAL * HEAD_DIM)

def reference(tokens, norm_gain_attn, w_query, w_key, w_value, w_forget, forget_bias, cache_keys, cache_values, cache_logcum, lengths, w_out, norm_gain_mix, norm_gain_ffn, expert_gate, expert_up, expert_down, routes, route_weights):
    residual = tokens.astype(jnp.float32)
    normed = rms_scaled(residual, norm_gain_attn).astype(jnp.bfloat16)
    query = jnp.dot(normed, w_query, preferred_element_type=jnp.float32).astype(jnp.bfloat16)
    new_keys = jnp.dot(normed, w_key, preferred_element_type=jnp.float32).astype(jnp.bfloat16)
    new_values = jnp.dot(normed, w_value, preferred_element_type=jnp.float32).astype(jnp.bfloat16)
    new_log_gate = jax.nn.log_sigmoid(jnp.dot(normed, w_forget, preferred_element_type=jnp.float32) + forget_bias)
    groups = SEQUENCE_TOTAL // B_DEV

    def by_group(array):
        return array.reshape((groups, B_DEV) + array.shape[1:])

    def one_group(items):
        return attend(*items)
    heads_out = lax.map(one_group, (by_group(query), by_group(new_keys), by_group(new_values), by_group(new_log_gate), by_group(cache_keys), by_group(cache_values), by_group(cache_logcum), by_group(lengths)))
    heads_out = heads_out.reshape(SEQUENCE_TOTAL, HEAD_TOTAL * HEAD_DIM)
    head_width = HEAD_TOTAL * HEAD_DIM // N_TP
    grouped_out = heads_out.astype(jnp.float32).reshape(SEQUENCE_TOTAL, N_TP, head_width)
    grouped_w = w_out.astype(jnp.float32).reshape(N_TP, head_width, D)
    partials = jnp.einsum('stc,tcd->tsd', grouped_out, grouped_w)
    partials = lax.optimization_barrier(partials.astype(jnp.bfloat16)).astype(jnp.float32)
    mix = lax.optimization_barrier(jnp.sum(partials, axis=0))
    mixed_res = residual + rms_scaled(mix, norm_gain_mix)
    ffn_in = rms_scaled(mixed_res, norm_gain_ffn).astype(jnp.bfloat16)

    def expert_step(carry, expert_index):
        start = expert_index * FF
        gate_part = jnp.dot(ffn_in, lax.dynamic_slice_in_dim(expert_gate, start, FF, 1), preferred_element_type=jnp.float32)
        up_part = jnp.dot(ffn_in, lax.dynamic_slice_in_dim(expert_up, start, FF, 1), preferred_element_type=jnp.float32)
        hidden = (jax.nn.silu(gate_part) * up_part).astype(jnp.bfloat16)
        expert_out = jnp.dot(hidden, lax.dynamic_slice_in_dim(expert_down, start, FF, 0), preferred_element_type=jnp.float32)
        weight = lax.optimization_barrier(jnp.sum(jnp.where(routes == expert_index, route_weights, 0.0), axis=1))
        return (carry + weight[:, None] * expert_out, None)
    routed, _ = lax.scan(expert_step, jnp.zeros((SEQUENCE_TOTAL, D), jnp.float32), jnp.arange(EXPERTS, dtype=jnp.int32))
    layer_out = (mixed_res + routed).astype(jnp.bfloat16)
    return (layer_out, new_keys, new_values, new_log_gate)
```

```python
import jax
import jax.numpy as jnp
from jax import lax
from jax.sharding import Mesh, PartitionSpec as P

HEAD_TOTAL = 32
KV_HEADS = 4
HEAD_DIM = 64
TOP = 2
EXPERTS = 16
CAP = 8
EPSILON = 1e-06
MASKED = -1e30
EP = ("z", "x", "c")
F32 = jnp.float32
BF16 = jnp.bfloat16


def shifted(value, axis, step):
    n = lax.axis_size(axis)
    return lax.ppermute(value, axis, [(i, (i + step) % n) for i in range(n)])


def exchange(blocks, axis):
    return lax.all_to_all(blocks, axis, split_axis=0, concat_axis=0, tiled=True)


def inv_rms(field):
    return lax.rsqrt(jnp.mean(field * field, axis=-1, keepdims=True) + EPSILON)


def body(
    tokens,
    norm_gain_attn,
    w_query,
    w_key,
    w_value,
    w_forget,
    forget_bias,
    cache_keys,
    cache_values,
    cache_logcum,
    lengths,
    w_out,
    norm_gain_mix,
    norm_gain_ffn,
    expert_gate,
    expert_up,
    expert_down,
    routes,
    route_weights,
):
    rows, width = tokens.shape
    query_cols = w_query.shape[1]
    key_cols = w_key.shape[1]
    nz, nx, nc, ny = (lax.axis_size(a) for a in ("z", "x", "c", "y"))
    iz, ic, iy = lax.axis_index("z"), lax.axis_index("c"), lax.axis_index("y")
    depth = width // nz

    weights = jnp.concatenate((w_query, w_key, w_value), axis=1)
    cols = weights.shape[1]
    weights = exchange(jnp.broadcast_to(weights, (nx * nc, *weights.shape)), ("x", "c"))
    weights = weights.reshape(depth, cols)
    gain_cols = lax.dynamic_slice_in_dim(norm_gain_attn, iz * depth, depth, 0)
    part_tokens = exchange(jnp.transpose(tokens.reshape(rows, nz, depth), (1, 0, 2)), "z")
    part_tokens = (part_tokens.astype(F32) * gain_cols).astype(BF16).reshape(nz * rows, depth)
    partial = jnp.dot(part_tokens, weights, preferred_element_type=F32).astype(BF16)
    arrived = exchange(partial.reshape(nz, rows, cols), "z")

    residual = tokens.astype(F32)
    scale_attn = inv_rms(residual)
    normed = (residual * scale_attn * norm_gain_attn).astype(BF16)
    new_log_gate = jax.nn.log_sigmoid(
        jnp.dot(normed, w_forget, preferred_element_type=F32) + forget_bias
    )
    projected = jnp.sum(arrived.astype(F32), axis=0) * scale_attn
    query = projected[:, :query_cols].astype(BF16)
    new_keys = projected[:, query_cols : query_cols + key_cols].astype(BF16)
    new_values = projected[:, query_cols + key_cols :].astype(BF16)

    local_heads = query_cols // HEAD_DIM
    local_kv = key_cols // HEAD_DIM
    group = HEAD_TOTAL // KV_HEADS
    span_len = cache_keys.shape[2]
    scale = HEAD_DIM ** (-0.5)
    query_heads = query.reshape(rows, local_kv, group, HEAD_DIM)
    key_heads = cache_keys.reshape(rows, local_kv, HEAD_DIM, span_len)
    value_heads = cache_values.reshape(rows, local_kv, HEAD_DIM, span_len)
    scores = jnp.einsum("bkgd,bkdl->bkgl", query_heads, key_heads, preferred_element_type=F32)
    scores = scores.reshape(rows, local_heads, span_len) * scale
    own_key = new_keys.astype(F32).reshape(rows, local_kv, 1, HEAD_DIM)
    own_score = (
        jnp.sum(query_heads.astype(F32) * own_key, axis=-1).reshape(rows, local_heads) * scale
    )
    places = jnp.arange(span_len, dtype=jnp.int32)
    at_last = (places[None, :] == (lengths - 1)[:, None]).astype(F32)
    last_cum = jnp.sum(cache_logcum * at_last[:, None, :], axis=2)
    shift = (last_cum + new_log_gate)[:, :, None] - cache_logcum
    valid = (places[None, :] < lengths[:, None])[:, None, :]
    past = jnp.where(valid, scores + shift, MASKED)
    peak = jnp.maximum(jnp.max(past, axis=-1), own_score)
    past_exp = jnp.exp(past - peak[:, :, None])
    own_exp = jnp.exp(own_score - peak)
    total = jnp.sum(past_exp, axis=-1) + own_exp
    past_weight = (
        (past_exp / total[:, :, None]).astype(BF16).reshape(rows, local_kv, group, span_len)
    )
    own_weight = (own_exp / total).astype(BF16).astype(F32).reshape(rows, local_kv, group)
    mixed = jnp.einsum("bkgl,bkdl->bkgd", past_weight, value_heads, preferred_element_type=F32)
    own_value = new_values.astype(F32).reshape(rows, local_kv, 1, HEAD_DIM)
    mixed = mixed + own_weight[:, :, :, None] * own_value
    heads_out = mixed.astype(BF16).reshape(rows, query_cols)

    partial_mix = jnp.dot(heads_out, w_out, preferred_element_type=F32).astype(BF16)
    others = [shifted(partial_mix, "y", s) for s in range(1, ny)]
    mix = partial_mix.astype(F32)
    for other in others:
        mix = mix + other.astype(F32)
    mixed_res = residual + mix * inv_rms(mix) * norm_gain_mix
    col_width = width // ny
    half = col_width // nc
    scale_ffn = inv_rms(mixed_res)
    residual_cols = lax.dynamic_slice_in_dim(mixed_res, iy * col_width, col_width, 1)
    gain_ffn_cols = lax.dynamic_slice_in_dim(norm_gain_ffn, iy * col_width, col_width, 0)
    ffn_cols = (residual_cols * scale_ffn * gain_ffn_cols).astype(BF16)

    flat_routes = routes.reshape(-1)
    expert_hits = (
        flat_routes[:, None] == jnp.arange(EXPERTS, dtype=jnp.int32)[None, :]
    ).astype(jnp.int32)
    earlier = jnp.cumsum(expert_hits, axis=0) - expert_hits
    slot_index = jnp.sum(earlier * expert_hits, axis=1)
    in_slot = (slot_index[:, None] == jnp.arange(CAP, dtype=jnp.int32)[None, :]).astype(F32)
    placing = expert_hits.astype(F32)[:, :, None] * in_slot[:, None, :]
    placing = placing.reshape(rows, TOP, EXPERTS * CAP)
    selector = jnp.sum(placing, axis=1).astype(BF16)
    weighing = jnp.sum(placing * route_weights[:, :, None], axis=1)

    packed = jnp.einsum("ra,rd->ad", selector, ffn_cols, preferred_element_type=F32).astype(BF16)
    pairs = nx * nz // EXPERTS
    packed = packed.reshape(nz, EXPERTS // nz, 1, CAP, nc, half).transpose(0, 1, 2, 4, 3, 5)
    outgoing = jnp.broadcast_to(packed, (nz, EXPERTS // nz, pairs, nc, CAP, half))
    arrived_rows = exchange(outgoing.reshape(nz * nx * nc, CAP, half), EP)
    count = nz * nx * nc * CAP
    own_rows = arrived_rows.reshape(count, half)
    pieces = [own_rows] + [shifted(own_rows, "y", s) for s in range(1, ny)]
    own_side = jnp.concatenate(pieces, axis=1)
    other_side = shifted(own_side, "c", 1)

    def row_blocks(w, side):
        blocks = w.reshape(ny, nc, half, w.shape[1])
        return [
            lax.dynamic_slice(blocks, ((iy - s) % ny, side, 0, 0), (1, 1, half, w.shape[1]))[0, 0]
            for s in range(ny)
        ]

    def rows_in_order(w):
        return (
            jnp.concatenate(row_blocks(w, ic), axis=0),
            jnp.concatenate(row_blocks(w, 1 - ic), axis=0),
        )

    gate_own, gate_other = rows_in_order(expert_gate)
    up_own, up_other = rows_in_order(expert_up)
    gate_part = jnp.dot(own_side, gate_own, preferred_element_type=F32) + jnp.dot(
        other_side, gate_other, preferred_element_type=F32
    )
    up_part = jnp.dot(own_side, up_own, preferred_element_type=F32) + jnp.dot(
        other_side, up_other, preferred_element_type=F32
    )
    hidden = (jax.nn.silu(gate_part) * up_part).astype(BF16)

    down_blocks = expert_down.reshape(expert_down.shape[0], ny, nc, half)

    def down_cols(side):
        return jnp.concatenate(
            [
                lax.dynamic_slice(
                    down_blocks, (0, (iy + s) % ny, side, 0), (down_blocks.shape[0], 1, 1, half)
                )[:, 0, 0]
                for s in range(ny)
            ],
            axis=1,
        )

    for_other = jnp.dot(hidden, down_cols(1 - ic), preferred_element_type=F32).astype(BF16)
    from_other = shifted(for_other, "c", 1)
    summed = jnp.dot(hidden, down_cols(ic), preferred_element_type=F32) + from_other.astype(F32)
    back = [
        shifted(summed[:, s * half : (s + 1) * half].astype(BF16), "y", s) for s in range(1, ny)
    ]
    total_rows = summed[:, :half]
    for piece in back:
        total_rows = total_rows + piece.astype(F32)
    returned = exchange(total_rows.astype(BF16).reshape(nz * nx * nc, CAP, half), EP)

    spread = jnp.broadcast_to(
        weighing.reshape(rows, nz, EXPERTS // nz, 1, CAP), (rows, nz, EXPERTS // nz, pairs, CAP)
    ).reshape(rows, nz * nx * CAP)
    returned = returned.reshape(nz * nx, nc, CAP, half).transpose(0, 2, 1, 3)
    returned = returned.reshape(nz * nx * CAP, nc * half)
    routed = jnp.dot(spread, returned.astype(F32), preferred_element_type=F32)
    layer_out = (residual_cols + routed).astype(BF16)
    return (layer_out, new_keys, new_values, new_log_gate)


def solution(mesh):
    chips = Mesh(mesh.devices.reshape(8, 4, 2, 4), ("z", "x", "c", "y"))
    everyone = ("z", "x", "c", "y")
    placed = (
        P(EP, None),
        P(),
        P(EP, "y"),
        P(EP, "y"),
        P(EP, "y"),
        P(None, "y"),
        P("y"),
        P(EP, "y", None),
        P(EP, "y", None),
        P(EP, "y", None),
        P(EP),
        P("y", None),
        P(),
        P(),
        P(None, everyone),
        P(None, everyone),
        P(everyone, None),
        P(EP, None),
        P(EP, None),
    )
    return jax.shard_map(
        body,
        mesh=chips,
        in_specs=placed,
        out_specs=(P(EP, "y"), P(EP, "y"), P(EP, "y"), P(EP, "y")),
        check_vma=False,
    )
```

```python
import functools

import jax
import jax.numpy as jnp
from jax import lax
from jax.experimental import pallas as pl
from jax.experimental.pallas import tpu as pltpu
from jax.sharding import Mesh, PartitionSpec as P

HEAD_TOTAL = 32
KV_HEADS = 4
HEAD_DIM = 64
TOP = 2
EXPERTS = 16
CAP = 8
EPSILON = 1e-06
MASKED = -1e30
EP = ("z", "x", "c")
F32 = jnp.float32
BF16 = jnp.bfloat16


def shifted(value, axis, step):
    n = lax.axis_size(axis)
    return lax.ppermute(value, axis, [(i, (i + step) % n) for i in range(n)])


def exchange(blocks, axis):
    return lax.all_to_all(blocks, axis, split_axis=0, concat_axis=0, tiled=True)


def inv_rms(field):
    return lax.rsqrt(jnp.mean(field * field, axis=-1, keepdims=True) + EPSILON)


def expert_kernel(nx, rows_ref, gate_ref, up_ref, down_ref, out_ref):
    blocks, part, width = rows_ref.shape
    ny = blocks // nx
    gate = up = None
    for y in range(ny):
        taken = jnp.concatenate([rows_ref[x * ny + y] for x in range(nx)], axis=0)
        deep = pl.ds(y * width, width)
        g = jnp.dot(taken, gate_ref[deep, :], preferred_element_type=F32)
        u = jnp.dot(taken, up_ref[deep, :], preferred_element_type=F32)
        gate, up = (g, u) if gate is None else (gate + g, up + u)
    hidden = (gate / (1.0 + jnp.exp(-gate)) * up).astype(BF16)
    for y in range(ny):
        back = jnp.dot(hidden, down_ref[:, pl.ds(y * width, width)], preferred_element_type=F32)
        back = back.astype(BF16)
        for x in range(nx):
            out_ref[x * ny + y] = back[x * part : (x + 1) * part]


def expert_rows(blocks, gate, up, down, nx):
    return pl.pallas_call(
        functools.partial(expert_kernel, nx),
        out_shape=jax.ShapeDtypeStruct(blocks.shape, BF16),
        in_specs=[pl.BlockSpec(memory_space=pltpu.VMEM)] * 4,
        out_specs=pl.BlockSpec(memory_space=pltpu.VMEM),
        cost_estimate=pl.CostEstimate(
            flops=2 * blocks.size * 3 * gate.shape[1],
            bytes_accessed=4 * blocks.size + 6 * gate.size,
            transcendentals=0,
        ),
    )(blocks, gate, up, down)


def body(
    tokens,
    norm_gain_attn,
    w_query,
    w_key,
    w_value,
    w_forget,
    forget_bias,
    cache_keys,
    cache_values,
    cache_logcum,
    lengths,
    w_out,
    norm_gain_mix,
    norm_gain_ffn,
    expert_gate,
    expert_up,
    expert_down,
    routes,
    route_weights,
):
    rows, width = tokens.shape
    query_cols = w_query.shape[1]
    key_cols = w_key.shape[1]
    nz, nx, nc, ny = (lax.axis_size(a) for a in ("z", "x", "c", "y"))
    ix, ic, iy = lax.axis_index("x"), lax.axis_index("c"), lax.axis_index("y")

    weights = jnp.concatenate((w_query, w_key, w_value), axis=1)
    cols = weights.shape[1]
    same_core = exchange(jnp.broadcast_to(weights, (nz, *weights.shape)), "z")
    other_core = shifted(same_core, "c", 1)
    first = ic == 0
    weights = jnp.stack(
        (jnp.where(first, same_core, other_core), jnp.where(first, other_core, same_core)), axis=1
    ).reshape(width // nx, cols)
    chunk = width // (nz * nx)
    scaled = (tokens.astype(F32) * norm_gain_attn).astype(BF16)
    scaled = scaled.reshape(rows, nz, nx, chunk).transpose(2, 0, 1, 3).reshape(nx, rows, nz * chunk)
    mine = [
        lax.dynamic_index_in_dim(scaled, (ix + s) % nx, 0, keepdims=False) for s in range(nx)
    ]
    part_tokens = jnp.concatenate(
        [mine[0]] + [shifted(mine[s], "x", s) for s in range(1, nx)], axis=0
    )
    partial = jnp.dot(part_tokens, weights, preferred_element_type=F32)
    projected = partial[:rows]
    for s in range(1, nx):
        piece = partial[s * rows : (s + 1) * rows].astype(BF16)
        projected = projected + shifted(piece, "x", nx - s).astype(F32)

    residual = tokens.astype(F32)
    scale_attn = inv_rms(residual)
    normed = (residual * scale_attn * norm_gain_attn).astype(BF16)
    new_log_gate = jax.nn.log_sigmoid(
        jnp.dot(normed, w_forget, preferred_element_type=F32) + forget_bias
    )
    projected = projected * scale_attn
    query = projected[:, :query_cols].astype(BF16)
    new_keys = projected[:, query_cols : query_cols + key_cols].astype(BF16)
    new_values = projected[:, query_cols + key_cols :].astype(BF16)

    local_heads = query_cols // HEAD_DIM
    local_kv = key_cols // HEAD_DIM
    group = HEAD_TOTAL // KV_HEADS
    span_len = cache_keys.shape[2]
    scale = HEAD_DIM ** (-0.5)
    query_heads = query.reshape(rows, local_kv, group, HEAD_DIM)
    key_heads = cache_keys.reshape(rows, local_kv, HEAD_DIM, span_len)
    value_heads = cache_values.reshape(rows, local_kv, HEAD_DIM, span_len)
    scores = jnp.einsum("bkgd,bkdl->bkgl", query_heads, key_heads, preferred_element_type=F32)
    scores = scores.reshape(rows, local_heads, span_len) * scale
    own_key = new_keys.astype(F32).reshape(rows, local_kv, 1, HEAD_DIM)
    own_score = (
        jnp.sum(query_heads.astype(F32) * own_key, axis=-1).reshape(rows, local_heads) * scale
    )
    places = jnp.arange(span_len, dtype=jnp.int32)
    at_last = (places[None, :] == (lengths - 1)[:, None]).astype(F32)
    last_cum = jnp.sum(cache_logcum * at_last[:, None, :], axis=2)
    shift = (last_cum + new_log_gate)[:, :, None] - cache_logcum
    valid = (places[None, :] < lengths[:, None])[:, None, :]
    past = jnp.where(valid, scores + shift, MASKED)
    peak = jnp.maximum(jnp.max(past, axis=-1), own_score)
    past_exp = jnp.exp(past - peak[:, :, None])
    own_exp = jnp.exp(own_score - peak)
    total = jnp.sum(past_exp, axis=-1) + own_exp
    past_weight = (
        (past_exp / total[:, :, None]).astype(BF16).reshape(rows, local_kv, group, span_len)
    )
    own_weight = (own_exp / total).astype(BF16).astype(F32).reshape(rows, local_kv, group)
    mixed = jnp.einsum("bkgl,bkdl->bkgd", past_weight, value_heads, preferred_element_type=F32)
    own_value = new_values.astype(F32).reshape(rows, local_kv, 1, HEAD_DIM)
    mixed = mixed + own_weight[:, :, :, None] * own_value
    heads_out = mixed.astype(BF16).reshape(rows, query_cols)

    partial_mix = jnp.dot(heads_out, w_out, preferred_element_type=F32).astype(BF16)
    others = [shifted(partial_mix, "y", s) for s in range(1, ny)]
    mix = partial_mix.astype(F32)
    for other in others:
        mix = mix + other.astype(F32)
    mixed_res = residual + mix * inv_rms(mix) * norm_gain_mix
    col_width = width // ny
    scale_ffn = inv_rms(mixed_res)
    residual_cols = lax.dynamic_slice_in_dim(mixed_res, iy * col_width, col_width, 1)
    gain_ffn_cols = lax.dynamic_slice_in_dim(norm_gain_ffn, iy * col_width, col_width, 0)
    ffn_cols = (residual_cols * scale_ffn * gain_ffn_cols).astype(BF16)

    flat_routes = routes.reshape(-1)
    expert_hits = (
        flat_routes[:, None] == jnp.arange(EXPERTS, dtype=jnp.int32)[None, :]
    ).astype(jnp.int32)
    earlier = jnp.cumsum(expert_hits, axis=0) - expert_hits
    slot_index = jnp.sum(earlier * expert_hits, axis=1)
    in_slot = (slot_index[:, None] == jnp.arange(CAP, dtype=jnp.int32)[None, :]).astype(F32)
    placing = expert_hits.astype(F32)[:, :, None] * in_slot[:, None, :]
    placing = placing.reshape(rows, TOP, EXPERTS * CAP)
    selector = jnp.sum(placing, axis=1).astype(BF16)
    weighing = jnp.sum(placing * route_weights[:, :, None], axis=1)

    packed = jnp.einsum("ra,rd->ad", selector, ffn_cols, preferred_element_type=F32).astype(BF16)
    local_experts = EXPERTS // nz
    spread = nx // local_experts
    on_z = exchange(packed.reshape(nz, local_experts * CAP, col_width), "z")
    on_z = on_z.reshape(nz, local_experts, CAP, col_width).transpose(1, 0, 2, 3)
    on_z = on_z.reshape(local_experts, 1, 1, nz * CAP, col_width)
    outgoing = jnp.broadcast_to(on_z, (local_experts, spread, ny, nz * CAP, col_width))
    own = exchange(outgoing.reshape(nx * ny, nz * CAP, col_width), ("x", "y"))
    other = shifted(own, "c", 1)
    own_part = expert_rows(own, expert_gate, expert_up, expert_down, nx)
    other_part = expert_rows(other, expert_gate, expert_up, expert_down, nx)
    both = own_part.astype(F32) + shifted(other_part, "c", 1).astype(F32)
    summed = exchange(both.astype(BF16), ("x", "y"))
    summed = summed.reshape(local_experts, spread * ny, nz, CAP, col_width).astype(F32)
    summed = jnp.sum(summed, axis=1).astype(BF16).transpose(1, 0, 2, 3)
    returned = exchange(summed.reshape(nz, local_experts * CAP, col_width), "z")
    returned = returned.reshape(EXPERTS * CAP, col_width)
    routed = jnp.dot(weighing, returned.astype(F32), preferred_element_type=F32)
    layer_out = (residual_cols + routed).astype(BF16)
    return (layer_out, new_keys, new_values, new_log_gate)


def solution(mesh):
    chips = Mesh(mesh.devices.reshape(8, 4, 2, 4), ("z", "x", "c", "y"))
    everyone = ("z", "x", "c", "y")
    placed = (
        P(EP, None),
        P(),
        P(EP, "y"),
        P(EP, "y"),
        P(EP, "y"),
        P(None, "y"),
        P("y"),
        P(EP, "y", None),
        P(EP, "y", None),
        P(EP, "y", None),
        P(EP),
        P("y", None),
        P(),
        P(),
        P(None, everyone),
        P(None, everyone),
        P(everyone, None),
        P(EP, None),
        P(EP, None),
    )
    return jax.shard_map(
        body,
        mesh=chips,
        in_specs=placed,
        out_specs=(P(EP, "y"), P(EP, "y"), P(EP, "y"), P(EP, "y")),
        check_vma=False,
    )
```

```python
import functools

import jax
import jax.numpy as jnp
from jax import lax
from jax.experimental import pallas as pl
from jax.experimental.pallas import tpu as pltpu
from jax.sharding import Mesh, PartitionSpec as P


HEAD_DIM = 64
EXPERTS = 16
CAP = 8
EPSILON = 1e-06
MASKED = -1e30
EP = ("z", "x", "c")
F32 = jnp.float32
BF16 = jnp.bfloat16


def shifted(value, axis, step):
    n = lax.axis_size(axis)
    return lax.ppermute(value, axis, [(i, (i + step) % n) for i in range(n)])


def exchange(blocks, axis):
    return lax.all_to_all(blocks, axis, split_axis=0, concat_axis=0, tiled=True)


def inv_rms(field):
    return lax.rsqrt(jnp.mean(field * field, axis=-1, keepdims=True) + EPSILON)


def expert_kernel(nx, rows_ref, gate_ref, up_ref, down_ref, out_ref):
    blocks, part, width = rows_ref.shape
    ny = blocks // nx
    gate = up = None
    for y in range(ny):
        taken = jnp.concatenate([rows_ref[x * ny + y] for x in range(nx)], axis=0)
        deep = pl.ds(y * width, width)
        g = jnp.dot(taken, gate_ref[deep, :], preferred_element_type=F32)
        u = jnp.dot(taken, up_ref[deep, :], preferred_element_type=F32)
        gate, up = (g, u) if gate is None else (gate + g, up + u)
    hidden = (gate / (1.0 + jnp.exp(-gate)) * up).astype(BF16)
    for y in range(ny):
        back = jnp.dot(hidden, down_ref[:, pl.ds(y * width, width)], preferred_element_type=F32)
        back = back.astype(BF16)
        for x in range(nx):
            out_ref[x * ny + y] = back[x * part : (x + 1) * part]


def expert_rows(blocks, gate, up, down, nx):
    return pl.pallas_call(
        functools.partial(expert_kernel, nx),
        out_shape=jax.ShapeDtypeStruct(blocks.shape, BF16),
        in_specs=[pl.BlockSpec(memory_space=pltpu.VMEM)] * 4,
        out_specs=pl.BlockSpec(memory_space=pltpu.VMEM),
        compiler_params=pltpu.CompilerParams(vmem_limit_bytes=16 * 2**20),
        cost_estimate=pl.CostEstimate(
            flops=2 * blocks.size * 3 * gate.shape[1],
            bytes_accessed=4 * blocks.size + 6 * gate.size,
            transcendentals=0,
        ),
    )(blocks, gate, up, down)


def attend_kernel(
    together,
    tokens_ref,
    gain_ref,
    forget_ref,
    bias_ref,
    own_ref,
    pieces_refs,
    cum_ref,
    length_ref,
    keys_ref,
    values_ref,
    out_w_ref,
    mix_ref,
    key_ref,
    value_ref,
    gate_ref,
    q_s,
    own_s,
    gate_s,
    weight_s,
    heads_s,
    keys_s,
    values_s,
    sems,
):
    rows = tokens_ref.shape[0]
    _, head_dim, span_len = keys_ref.shape
    _, group, _ = q_s.shape
    cols = group * head_dim
    scale = HEAD_DIM ** (-0.5)
    copies = []
    for step in range(rows // together):
        some = pl.ds(step * together, together)
        copies.append(
            (
                pltpu.make_async_copy(keys_ref.at[some], keys_s.at[some], sems.at[0, step]),
                pltpu.make_async_copy(values_ref.at[some], values_s.at[some], sems.at[1, step]),
            )
        )
        for copy in copies[step]:
            copy.start()

    tokens = tokens_ref[...].astype(F32)
    scale_attn = lax.rsqrt(jnp.mean(tokens * tokens, axis=1, keepdims=True) + EPSILON)
    normed = (tokens * scale_attn * gain_ref[...]).astype(BF16)
    logits = lax.dot_general(
        normed, forget_ref[...], (((1,), (1,)), ((), ())), preferred_element_type=F32
    )
    logits = logits + bias_ref[...]
    gate = jnp.minimum(logits, 0.0) - jnp.log1p(jnp.exp(-jnp.abs(logits)))
    gate_ref[...] = gate
    projected = own_ref[...]
    for ref in pieces_refs:
        projected = projected + ref[...].astype(F32)
    projected = projected * scale_attn
    new_key = projected[:, cols : cols + head_dim].astype(BF16)
    new_value = projected[:, cols + head_dim : cols + 2 * head_dim].astype(BF16)
    key_ref[...] = new_key
    value_ref[...] = new_value

    query = projected[:, :cols].astype(BF16).astype(F32)
    at_head = lax.broadcasted_iota(jnp.int32, (rows, group, cols), 1)
    of_head = lax.shift_right_logical(
        lax.broadcasted_iota(jnp.int32, (rows, group, cols), 2), head_dim.bit_length() - 1
    )
    on_head = at_head == of_head
    spread = jnp.where(on_head, jnp.broadcast_to(query[:, None, :], (rows, group, cols)), 0.0)
    spread = spread.reshape(rows * group, cols).astype(BF16)
    fold = (
        lax.bitwise_and(lax.broadcasted_iota(jnp.int32, (cols, head_dim), 0), head_dim - 1)
        == lax.broadcasted_iota(jnp.int32, (cols, head_dim), 1)
    )
    fold = jnp.where(fold, 1.0, 0.0).astype(BF16)
    by_head = jnp.dot(spread, fold, preferred_element_type=F32).reshape(rows, group, head_dim)
    q_s[...] = by_head
    own_s[...] = (
        jnp.sum(by_head * new_key.astype(F32)[:, None, :], axis=2, keepdims=True) * scale
    )
    same = lax.broadcasted_iota(jnp.int32, (rows, group, group), 1) == lax.broadcasted_iota(
        jnp.int32, (rows, group, group), 2
    )
    gate_s[...] = jnp.sum(jnp.where(same, gate[:, None, :], 0.0), axis=2, keepdims=True)
    places = lax.broadcasted_iota(jnp.int32, (group, span_len), 1)

    for step in range(rows // together):
        for copy in copies[step]:
            copy.wait()
        for k in range(together):
            b = step * together + k
            length = length_ref[b]
            scores = jnp.dot(q_s[b].astype(BF16), keys_s[b], preferred_element_type=F32) * scale
            cum = cum_ref[b]
            last = jnp.sum(jnp.where(places == length - 1, cum, 0.0), axis=1, keepdims=True)
            past = jnp.where(places < length, scores + ((last + gate_s[b]) - cum), MASKED)
            own = own_s[b]
            peak = jnp.maximum(jnp.max(past, axis=1, keepdims=True), own)
            past_exp = jnp.exp(past - peak)
            own_exp = jnp.exp(own - peak)
            total = jnp.sum(past_exp, axis=1, keepdims=True) + own_exp
            weight = (past_exp / total).astype(BF16)
            weight_s[b] = own_exp / total
            heads_s[b] = lax.dot_general(
                weight, values_s[b], (((1,), (1,)), ((), ())), preferred_element_type=F32
            )
    own_weight = weight_s[...].astype(BF16).astype(F32)
    heads = heads_s[...] + own_weight * new_value.astype(F32)[:, None, :]
    heads = heads.reshape(rows * group, head_dim).astype(BF16)
    wide = lax.dot_general(heads, fold, (((1,), (1,)), ((), ())), preferred_element_type=F32)
    wide = jnp.where(on_head, wide.reshape(rows, group, cols), 0.0)
    heads_out = jnp.sum(wide, axis=1).astype(BF16)
    mix_ref[...] = jnp.dot(heads_out, out_w_ref[...], preferred_element_type=F32).astype(BF16)


def attend(tokens, gain, forget, bias, own, pieces, cum, lengths, keys, values, out_w):
    rows, width = tokens.shape
    group, head_dim = cum.shape[1], keys.shape[1]
    in_vmem = pl.BlockSpec(memory_space=pltpu.VMEM)
    in_smem = pl.BlockSpec(memory_space=pltpu.SMEM)
    in_hbm = pl.BlockSpec(memory_space=pltpu.HBM)
    one = jax.ShapeDtypeStruct((rows, head_dim), BF16)
    together = 8
    return pl.pallas_call(
        functools.partial(attend_kernel, together),
        out_shape=(
            jax.ShapeDtypeStruct((rows, width), BF16),
            one,
            one,
            jax.ShapeDtypeStruct((rows, group), F32),
        ),
        in_specs=[in_vmem] * 5
        + [[in_vmem] * len(pieces), in_vmem, in_smem, in_hbm, in_hbm, in_vmem],
        out_specs=(in_vmem,) * 4,
        scratch_shapes=[
            pltpu.VMEM((rows, group, head_dim), F32),
            pltpu.VMEM((rows, group, 1), F32),
            pltpu.VMEM((rows, group, 1), F32),
            pltpu.VMEM((rows, group, 1), F32),
            pltpu.VMEM((rows, group, head_dim), F32),
            pltpu.VMEM(keys.shape, BF16),
            pltpu.VMEM(values.shape, BF16),
            pltpu.SemaphoreType.DMA((2, rows // together)),
        ],
        compiler_params=pltpu.CompilerParams(vmem_limit_bytes=24 * 2**20),
        cost_estimate=pl.CostEstimate(
            flops=4 * keys.size * group + 2 * rows * out_w.size,
            bytes_accessed=4 * keys.size + 4 * cum.size + 2 * out_w.size,
            transcendentals=cum.size,
        ),
    )(tokens, gain, forget, bias, own, pieces, cum, lengths, keys, values, out_w)


def slots_kernel(routes_ref, weights_ref, selector_ref, weighing_ref):
    top, rows = routes_ref.shape
    named = [routes_ref[pl.ds(k, 1), :] for k in range(top)]
    experts = lax.broadcasted_iota(jnp.int32, (EXPERTS, rows), 0)
    hits = [jnp.where(experts == one, 1.0, 0.0) for one in named]
    both = sum(hits[1:], hits[0])
    before = lax.broadcasted_iota(jnp.int32, (rows, rows), 0) < lax.broadcasted_iota(
        jnp.int32, (rows, rows), 1
    )
    earlier = jnp.dot(
        both.astype(BF16), jnp.where(before, 1.0, 0.0).astype(BF16), preferred_element_type=F32
    )
    places = lax.broadcasted_iota(jnp.int32, (EXPERTS * CAP, rows), 0)
    chosen = jnp.zeros((EXPERTS * CAP, rows), F32)
    weighed = jnp.zeros((EXPERTS * CAP, rows), F32)
    for k in range(top):
        slot = jnp.sum(earlier * hits[k], axis=0, keepdims=True).astype(jnp.int32)
        there = jnp.where(places == named[k] * CAP + slot, 1.0, 0.0)
        chosen = chosen + there
        weighed = weighed + there * weights_ref[pl.ds(k, 1), :]
    selector_ref[...] = chosen.astype(BF16)
    weighing_ref[...] = weighed


def slots(routes, weights):
    in_vmem = pl.BlockSpec(memory_space=pltpu.VMEM)
    shape = (EXPERTS * CAP, routes.shape[1])
    return pl.pallas_call(
        slots_kernel,
        out_shape=(jax.ShapeDtypeStruct(shape, BF16), jax.ShapeDtypeStruct(shape, F32)),
        in_specs=[in_vmem] * 2,
        out_specs=(in_vmem,) * 2,
        compiler_params=pltpu.CompilerParams(vmem_limit_bytes=4 * 2**20),
    )(routes, weights)


def layer(
    tokens,
    norm_gain_attn,
    w_query,
    w_key,
    w_value,
    w_forget,
    forget_bias,
    cache_keys,
    cache_values,
    cache_logcum,
    lengths,
    w_out,
    norm_gain_mix,
    norm_gain_ffn,
    expert_gate,
    expert_up,
    expert_down,
    routes,
    route_weights,
):
    rows, width = tokens.shape
    nz, nx, nc, ny = (lax.axis_size(a) for a in ("z", "x", "c", "y"))
    ix, ic, iy = lax.axis_index("x"), lax.axis_index("c"), lax.axis_index("y")

    selector, weighing = slots(routes.T, route_weights.T)

    weights = jnp.concatenate((w_query, w_key, w_value), axis=1)
    cols = weights.shape[1]
    same_core = exchange(jnp.broadcast_to(weights, (nz, *weights.shape)), "z")
    other_core = shifted(same_core, "c", 1)
    deep = width // (nx * nc)
    scaled = (tokens.astype(F32) * norm_gain_attn).astype(BF16)
    scaled = scaled.reshape(rows, nz, nx, nc, width // (nz * nx * nc)).transpose(2, 3, 0, 1, 4)
    scaled = scaled.reshape(nx, nc, rows, deep)
    mine = [
        jnp.concatenate(
            [
                lax.dynamic_slice(
                    scaled, ((ix + s) % nx, (ic + k) % nc, 0, 0), (1, 1, rows, deep)
                )[0, 0]
                for k in range(nc)
            ],
            axis=1,
        )
        for s in range(nx)
    ]
    moved = [shifted(mine[s], "x", s) for s in range(1, nx)]
    part_tokens = jnp.concatenate([mine[0]] + moved, axis=0)
    partial = jnp.dot(
        part_tokens[:, :deep], same_core.reshape(deep, cols), preferred_element_type=F32
    ) + jnp.dot(part_tokens[:, deep:], other_core.reshape(deep, cols), preferred_element_type=F32)
    pieces = [
        shifted(partial[s * rows : (s + 1) * rows].astype(BF16), "x", nx - s)
        for s in range(1, nx)
    ]

    partial_mix, new_keys, new_values, new_log_gate = attend(
        tokens,
        norm_gain_attn.reshape(1, width),
        w_forget.T,
        forget_bias.reshape(1, -1),
        partial[:rows],
        pieces,
        cache_logcum,
        lengths,
        pltpu.with_memory_space_constraint(cache_keys, pltpu.HBM),
        pltpu.with_memory_space_constraint(cache_values, pltpu.HBM),
        w_out,
    )

    residual = tokens.astype(F32)
    others = [shifted(partial_mix, "y", s) for s in range(1, ny)]
    mix = partial_mix.astype(F32)
    for other in others:
        mix = mix + other.astype(F32)
    mixed_res = residual + mix * inv_rms(mix) * norm_gain_mix
    col_width = width // ny
    scale_ffn = inv_rms(mixed_res)
    residual_cols = lax.dynamic_slice_in_dim(mixed_res, iy * col_width, col_width, 1)
    gain_ffn_cols = lax.dynamic_slice_in_dim(norm_gain_ffn, iy * col_width, col_width, 0)
    ffn_cols = (residual_cols * scale_ffn * gain_ffn_cols).astype(BF16)

    packed = jnp.dot(selector, ffn_cols, preferred_element_type=F32).astype(BF16)
    local_experts = EXPERTS // nz
    spread = nx // local_experts
    on_z = exchange(packed.reshape(nz, local_experts * CAP, col_width), "z")
    on_z = on_z.reshape(nz, local_experts, CAP, col_width).transpose(1, 0, 2, 3)
    on_z = on_z.reshape(local_experts, 1, 1, nz * CAP, col_width)
    outgoing = jnp.broadcast_to(on_z, (local_experts, spread, ny, nz * CAP, col_width))
    own = exchange(outgoing.reshape(nx * ny, nz * CAP, col_width), ("x", "y"))
    other = shifted(own, "c", 1)
    own_part = expert_rows(own, expert_gate, expert_up, expert_down, nx)
    other_part = expert_rows(other, expert_gate, expert_up, expert_down, nx)
    both = own_part.astype(F32) + shifted(other_part, "c", 1).astype(F32)
    summed = exchange(both.astype(BF16), ("x", "y"))
    summed = summed.reshape(local_experts, spread * ny, nz, CAP, col_width).astype(F32)
    summed = jnp.sum(summed, axis=1).astype(BF16).transpose(1, 0, 2, 3)
    returned = exchange(summed.reshape(nz, local_experts * CAP, col_width), "z")
    returned = returned.reshape(EXPERTS * CAP, col_width)
    routed = lax.dot_general(
        weighing, returned.astype(F32), (((0,), (0,)), ((), ())), preferred_element_type=F32
    )
    layer_out = (residual_cols + routed).astype(BF16)
    return (layer_out, new_keys, new_values, new_log_gate)


def solution(mesh):
    chips = Mesh(mesh.devices.reshape(8, 4, 2, 4), ("z", "x", "c", "y"))
    everyone = ("z", "x", "c", "y")
    placed = (
        P(EP, None),
        P(),
        P(EP, "y"),
        P(EP, "y"),
        P(EP, "y"),
        P(None, "y"),
        P("y"),
        P(EP, "y", None),
        P(EP, "y", None),
        P(EP, "y", None),
        P(EP),
        P("y", None),
        P(),
        P(),
        P(None, everyone),
        P(None, everyone),
        P(everyone, None),
        P(EP, None),
        P(EP, None),
    )
    return jax.shard_map(
        layer,
        mesh=chips,
        in_specs=placed,
        out_specs=(P(EP, "y"), P(EP, "y"), P(EP, "y"), P(EP, "y")),
        check_vma=False,
    )
```

```python
import functools

import jax
import jax.numpy as jnp
from jax import lax
from jax.experimental import pallas as pl
from jax.experimental.pallas import tpu as pltpu
from jax.sharding import Mesh, PartitionSpec as P


HEAD_DIM = 64
EXPERTS = 16
CAP = 8
EPSILON = 1e-06
MASKED = -1e30
EP = ("z", "x", "c")
F32 = jnp.float32
BF16 = jnp.bfloat16


def shifted(value, axis, step):
    n = lax.axis_size(axis)
    return lax.ppermute(value, axis, [(i, (i + step) % n) for i in range(n)])


def exchange(blocks, axis):
    return lax.all_to_all(blocks, axis, split_axis=0, concat_axis=0, tiled=True)


def inv_rms(field):
    return lax.rsqrt(jnp.mean(field * field, axis=-1, keepdims=True) + EPSILON)


def expert_kernel(nx, rows_ref, gate_ref, up_ref, down_ref, out_ref):
    blocks, part, width = rows_ref.shape
    ny = blocks // nx
    gate = up = None
    for y in range(ny):
        taken = jnp.concatenate([rows_ref[x * ny + y] for x in range(nx)], axis=0)
        deep = pl.ds(y * width, width)
        g = jnp.dot(taken, gate_ref[deep, :], preferred_element_type=F32)
        u = jnp.dot(taken, up_ref[deep, :], preferred_element_type=F32)
        gate, up = (g, u) if gate is None else (gate + g, up + u)
    hidden = (gate / (1.0 + jnp.exp(-gate)) * up).astype(BF16)
    for y in range(ny):
        back = jnp.dot(hidden, down_ref[:, pl.ds(y * width, width)], preferred_element_type=F32)
        back = back.astype(BF16)
        for x in range(nx):
            out_ref[x * ny + y] = back[x * part : (x + 1) * part]


def expert_rows(blocks, gate, up, down, nx):
    return pl.pallas_call(
        functools.partial(expert_kernel, nx),
        out_shape=jax.ShapeDtypeStruct(blocks.shape, BF16),
        in_specs=[pl.BlockSpec(memory_space=pltpu.VMEM)] * 4,
        out_specs=pl.BlockSpec(memory_space=pltpu.VMEM),
        compiler_params=pltpu.CompilerParams(vmem_limit_bytes=16 * 2**20),
        cost_estimate=pl.CostEstimate(
            flops=2 * blocks.size * 3 * gate.shape[1],
            bytes_accessed=4 * blocks.size + 6 * gate.size,
            transcendentals=0,
        ),
    )(blocks, gate, up, down)


def attend_kernel(
    together,
    parts,
    own_ref,
    pieces_refs,
    scale_ref,
    gate_ref,
    length_ref,
    cum_ref,
    keys_ref,
    values_ref,
    out_w_ref,
    mix_ref,
    key_ref,
    value_ref,
    q_s,
    own_s,
    weight_s,
    heads_s,
    past_s,
    cum_s,
    keys_s,
    values_s,
    out_w_s,
    sems,
):
    rows, group, head_dim = q_s.shape
    span_len = keys_ref.shape[2]
    cols = group * head_dim
    scale = HEAD_DIM ** (-0.5)
    share = rows // parts
    halves = [pl.ds(p * share, share) for p in range(parts)]

    def copies(number, source, target):
        return [
            pltpu.make_async_copy(source.at[h], target.at[h], sems.at[number, p])
            for p, h in enumerate(halves)
        ]

    key_copies = copies(0, keys_ref, keys_s)
    cum_copies = copies(1, cum_ref, cum_s)
    value_copies = copies(2, values_ref, values_s)
    out_w_copy = pltpu.make_async_copy(out_w_ref, out_w_s, sems.at[3, 0])
    for p in range(parts):
        cum_copies[p].start()
        key_copies[p].start()
    for copy in value_copies:
        copy.start()
    out_w_copy.start()

    projected = own_ref[...]
    for ref in pieces_refs:
        projected = projected + ref[...].astype(F32)
    projected = projected * scale_ref[...]
    new_key = projected[:, cols : cols + head_dim].astype(BF16)
    new_value = projected[:, cols + head_dim : cols + 2 * head_dim].astype(BF16)
    key_ref[...] = new_key
    value_ref[...] = new_value

    query = projected[:, :cols].astype(BF16).astype(F32)
    at_head = lax.broadcasted_iota(jnp.int32, (rows, group, cols), 1)
    of_head = lax.shift_right_logical(
        lax.broadcasted_iota(jnp.int32, (rows, group, cols), 2), head_dim.bit_length() - 1
    )
    on_head = at_head == of_head
    spread = jnp.where(on_head, jnp.broadcast_to(query[:, None, :], (rows, group, cols)), 0.0)
    spread = spread.reshape(rows * group, cols).astype(BF16)
    fold = (
        lax.bitwise_and(lax.broadcasted_iota(jnp.int32, (cols, head_dim), 0), head_dim - 1)
        == lax.broadcasted_iota(jnp.int32, (cols, head_dim), 1)
    )
    fold = jnp.where(fold, 1.0, 0.0).astype(BF16)
    by_head = jnp.dot(spread, fold, preferred_element_type=F32).reshape(rows, group, head_dim)
    q_s[...] = by_head
    own_s[...] = (
        jnp.sum(by_head * new_key.astype(F32)[:, None, :], axis=2, keepdims=True) * scale
    )
    places = lax.broadcasted_iota(jnp.int32, (group, span_len), 1)

    def weigh(some):
        scores = [
            jnp.dot(q_s[b].astype(BF16), keys_s[b], preferred_element_type=F32) * scale
            for b in some
        ]
        lengths = [length_ref[b] for b in some]
        cums = [cum_s[b] for b in some]
        lasts = [
            jnp.sum(jnp.where(places == n - 1, cum, 0.0), axis=1, keepdims=True)
            for n, cum in zip(lengths, cums)
        ]
        pasts = [
            jnp.where(places < n, score + ((last + gate_ref[b]) - cum), MASKED)
            for b, n, score, last, cum in zip(some, lengths, scores, lasts, cums)
        ]
        owns = [own_s[b] for b in some]
        peaks = [
            jnp.maximum(jnp.max(past, axis=1, keepdims=True), own)
            for past, own in zip(pasts, owns)
        ]
        past_exps = [jnp.exp(past - peak) for past, peak in zip(pasts, peaks)]
        own_exps = [jnp.exp(own - peak) for own, peak in zip(owns, peaks)]
        totals = [
            jnp.sum(past_exp, axis=1, keepdims=True) + own_exp
            for past_exp, own_exp in zip(past_exps, own_exps)
        ]
        for b, past_exp, own_exp, total in zip(some, past_exps, own_exps, totals):
            weight_s[b] = own_exp / total
            past_s[b] = (past_exp / total).astype(BF16)

    def mix(some):
        mixed = [
            lax.dot_general(
                past_s[b], values_s[b], (((1,), (1,)), ((), ())), preferred_element_type=F32
            )
            for b in some
        ]
        for b, one in zip(some, mixed):
            heads_s[b] = one

    for p in range(parts):
        cum_copies[p].wait()
        key_copies[p].wait()
        for first in range(p * share, (p + 1) * share, together):
            weigh(range(first, first + together))
    for p in range(parts):
        value_copies[p].wait()
        mix(range(p * share, (p + 1) * share))
    own_weight = weight_s[...].astype(BF16).astype(F32)
    heads = heads_s[...] + own_weight * new_value.astype(F32)[:, None, :]
    heads = heads.reshape(rows * group, head_dim).astype(BF16)
    wide = lax.dot_general(heads, fold, (((1,), (1,)), ((), ())), preferred_element_type=F32)
    wide = jnp.where(on_head, wide.reshape(rows, group, cols), 0.0)
    heads_out = jnp.sum(wide, axis=1).astype(BF16)
    out_w_copy.wait()
    mix_ref[...] = jnp.dot(heads_out, out_w_s[...], preferred_element_type=F32).astype(BF16)


def attend(own, pieces, scale, gate, lengths, cum, keys, values, out_w):
    rows, group, _ = cum.shape
    head_dim, width = keys.shape[1], out_w.shape[1]
    in_vmem = pl.BlockSpec(memory_space=pltpu.VMEM)
    from_hbm = pl.BlockSpec(memory_space=pltpu.HBM)
    one = jax.ShapeDtypeStruct((rows, head_dim), BF16)
    together, parts = 8, 2
    return pl.pallas_call(
        functools.partial(attend_kernel, together, parts),
        out_shape=(jax.ShapeDtypeStruct((rows, width), BF16), one, one),
        in_specs=[in_vmem, [in_vmem] * len(pieces)] + [in_vmem] * 3 + [from_hbm] * 4,
        out_specs=(in_vmem,) * 3,
        scratch_shapes=[
            pltpu.VMEM((rows, group, head_dim), F32),
            pltpu.VMEM((rows, group, 1), F32),
            pltpu.VMEM((rows, group, 1), F32),
            pltpu.VMEM((rows, group, head_dim), F32),
            pltpu.VMEM(cum.shape, BF16),
            pltpu.VMEM(cum.shape, F32),
            pltpu.VMEM(keys.shape, BF16),
            pltpu.VMEM(values.shape, BF16),
            pltpu.VMEM(out_w.shape, BF16),
            pltpu.SemaphoreType.DMA((4, parts)),
        ],
        compiler_params=pltpu.CompilerParams(vmem_limit_bytes=24 * 2**20),
        cost_estimate=pl.CostEstimate(
            flops=4 * keys.size * group + 2 * rows * out_w.size,
            bytes_accessed=4 * keys.size + 4 * cum.size + 2 * out_w.size,
            transcendentals=cum.size,
        ),
    )(own, pieces, scale, gate, lengths, *in_hbm(cum, keys, values, out_w))


def cut_kernel(nz, nx, *refs):
    outs, cut_s = refs[2 : 2 + nx], refs[2 + nx]
    tokens_ref, gain_ref = fetched(refs[:2], refs[3 + nx : -1], refs[-1])
    _, width = tokens_ref.shape
    chunk = width // (nz * nx)
    scaled = (tokens_ref[...].astype(F32) * gain_ref[...])
    for x in range(nx):
        cut_s[x] = jnp.concatenate(
            [scaled[:, (z * nx + x) * chunk : (z * nx + x + 1) * chunk] for z in range(nz)], axis=1
        )
    here = lax.axis_index("x")
    for s in range(nx):
        outs[s][...] = cut_s[lax.rem(here + s, nx)].astype(BF16)


def cut_tokens(tokens, gain, nz, nx):
    rows, width = tokens.shape
    in_vmem = pl.BlockSpec(memory_space=pltpu.VMEM)
    return pl.pallas_call(
        functools.partial(cut_kernel, nz, nx),
        out_shape=[jax.ShapeDtypeStruct((rows, width // nx), BF16)] * nx,
        in_specs=[pl.BlockSpec(memory_space=pltpu.HBM)] * 2,
        out_specs=[in_vmem] * nx,
        scratch_shapes=[pltpu.VMEM((nx, rows, width // nx), F32)] + places_for((tokens, gain)),
        compiler_params=pltpu.CompilerParams(vmem_limit_bytes=4 * 2**20),
    )(*in_hbm(tokens, gain))


def multiply_kernel(count, *refs):
    token_refs, (same_ref, other_ref), outs = refs[:count], refs[count : count + 2], refs[count + 2 :]
    first = lax.axis_index("c") == 0
    same, other = same_ref[...], other_ref[...]
    weights = jnp.concatenate(
        (jnp.where(first, same, other), jnp.where(first, other, same)), axis=1
    )
    weights = weights.reshape(-1, weights.shape[-1])
    tokens = jnp.concatenate([ref[...] for ref in token_refs], axis=0)
    product = jnp.dot(tokens, weights, preferred_element_type=F32)
    rows = token_refs[0].shape[0]
    for s, out in enumerate(outs):
        out[...] = product[s * rows : (s + 1) * rows].astype(out.dtype)


def multiply(pieces, same, other):
    rows = pieces[0].shape[0]
    cols = same.shape[2]
    in_vmem = pl.BlockSpec(memory_space=pltpu.VMEM)
    kinds = [F32] + [BF16] * (len(pieces) - 1)
    return pl.pallas_call(
        functools.partial(multiply_kernel, len(pieces)),
        out_shape=[jax.ShapeDtypeStruct((rows, cols), kind) for kind in kinds],
        in_specs=[in_vmem] * (len(pieces) + 2),
        out_specs=[in_vmem] * len(pieces),
        compiler_params=pltpu.CompilerParams(vmem_limit_bytes=8 * 2**20),
        cost_estimate=pl.CostEstimate(
            flops=4 * rows * len(pieces) * same.size,
            bytes_accessed=4 * same.size,
            transcendentals=0,
        ),
    )(*pieces, same, other)


def fetched(sources, targets, sems):
    copies = [
        pltpu.make_async_copy(source, target, sems.at[k])
        for k, (source, target) in enumerate(zip(sources, targets))
    ]
    for copy in copies:
        copy.start()
    for copy in copies:
        copy.wait()
    return targets


def in_hbm(*arrays):
    return [pltpu.with_memory_space_constraint(array, pltpu.HBM) for array in arrays]


def places_for(arrays):
    return [pltpu.VMEM(array.shape, array.dtype) for array in arrays] + [
        pltpu.SemaphoreType.DMA((len(arrays),))
    ]


def early_kernel(count, *refs):
    scale_ref, log_gate_ref, gate_ref, long_ref, selector_ref, weighing_ref = refs[count : count + 6]
    (
        tokens_ref,
        gain_ref,
        forget_ref,
        bias_ref,
        length_ref,
        routes_ref,
        weights_ref,
    ) = fetched(refs[:count], refs[count + 6 : -1], refs[-1])

    tokens = tokens_ref[...].astype(F32)
    rows = tokens.shape[0]
    group = forget_ref.shape[0]
    scale = lax.rsqrt(jnp.mean(tokens * tokens, axis=1, keepdims=True) + EPSILON)
    scale_ref[...] = scale
    normed = (tokens * scale * gain_ref[...]).astype(BF16)
    logits = lax.dot_general(
        normed, forget_ref[...], (((1,), (1,)), ((), ())), preferred_element_type=F32
    )
    logits = logits + bias_ref[...]
    gate = jnp.minimum(logits, 0.0) - jnp.log1p(jnp.exp(-jnp.abs(logits)))
    log_gate_ref[...] = gate
    same = lax.broadcasted_iota(jnp.int32, (rows, group, group), 1) == lax.broadcasted_iota(
        jnp.int32, (rows, group, group), 2
    )
    gate_ref[...] = jnp.sum(jnp.where(same, gate[:, None, :], 0.0), axis=2, keepdims=True)
    mine = lax.broadcasted_iota(jnp.int32, (rows, rows), 0) == lax.broadcasted_iota(
        jnp.int32, (rows, rows), 1
    )
    lengths = jnp.where(mine, length_ref[...].astype(F32), 0.0)
    lengths = jnp.sum(lengths, axis=1, keepdims=True)
    long_ref[...] = jnp.broadcast_to(lengths[:, None, :], long_ref.shape).astype(jnp.int32)

    top = routes_ref.shape[0]
    named = [routes_ref[pl.ds(k, 1), :] for k in range(top)]
    experts = lax.broadcasted_iota(jnp.int32, (EXPERTS, rows), 0)
    hits = [jnp.where(experts == one, 1.0, 0.0) for one in named]
    both = sum(hits[1:], hits[0])
    before = lax.broadcasted_iota(jnp.int32, (rows, rows), 0) < lax.broadcasted_iota(
        jnp.int32, (rows, rows), 1
    )
    earlier = jnp.dot(
        both.astype(BF16), jnp.where(before, 1.0, 0.0).astype(BF16), preferred_element_type=F32
    )
    places = lax.broadcasted_iota(jnp.int32, (EXPERTS * CAP, rows), 0)
    chosen = jnp.zeros((EXPERTS * CAP, rows), F32)
    weighed = jnp.zeros((EXPERTS * CAP, rows), F32)
    for k in range(top):
        slot = jnp.sum(earlier * hits[k], axis=0, keepdims=True).astype(jnp.int32)
        there = jnp.where(places == named[k] * CAP + slot, 1.0, 0.0)
        chosen = chosen + there
        weighed = weighed + there * weights_ref[pl.ds(k, 1), :]
    selector_ref[...] = chosen.astype(BF16)
    weighing_ref[...] = weighed


def early(*arrays):
    in_vmem = pl.BlockSpec(memory_space=pltpu.VMEM)
    tokens, _, forget, *_ = arrays
    rows, group = tokens.shape[0], forget.shape[0]
    slots = EXPERTS * CAP
    return pl.pallas_call(
        functools.partial(early_kernel, len(arrays)),
        out_shape=(
            jax.ShapeDtypeStruct((rows, 1), F32),
            jax.ShapeDtypeStruct((rows, group), F32),
            jax.ShapeDtypeStruct((rows, group, 1), F32),
            jax.ShapeDtypeStruct((rows, group, 1), jnp.int32),
            jax.ShapeDtypeStruct((slots, rows), BF16),
            jax.ShapeDtypeStruct((slots, rows), F32),
        ),
        in_specs=[pl.BlockSpec(memory_space=pltpu.HBM)] * len(arrays),
        out_specs=(in_vmem,) * 6,
        scratch_shapes=places_for(arrays),
        compiler_params=pltpu.CompilerParams(vmem_limit_bytes=6 * 2**20),
    )(*in_hbm(*arrays))


def layer(
    tokens,
    norm_gain_attn,
    w_query,
    w_key,
    w_value,
    w_forget,
    forget_bias,
    cache_keys,
    cache_values,
    cache_logcum,
    lengths,
    w_out,
    norm_gain_mix,
    norm_gain_ffn,
    expert_gate,
    expert_up,
    expert_down,
    routes,
    route_weights,
):
    _, width = tokens.shape
    nz, nx, _, ny = (lax.axis_size(a) for a in ("z", "x", "c", "y"))
    iy = lax.axis_index("y")

    scale_attn, new_log_gate, gate, long, selector, weighing = early(
        tokens,
        norm_gain_attn.reshape(1, width),
        w_forget.T,
        forget_bias.reshape(1, -1),
        lengths.reshape(1, -1),
        routes.T,
        route_weights.T,
    )

    weights = jnp.concatenate((w_query, w_key, w_value), axis=1)
    same_core = exchange(jnp.broadcast_to(weights, (nz, *weights.shape)), "z")
    other_core = shifted(same_core, "c", 1)
    mine = cut_tokens(tokens, norm_gain_attn.reshape(1, width), nz, nx)
    moved = [shifted(mine[s], "x", s) for s in range(1, nx)]
    own_partial, *partials = multiply([mine[0]] + moved, same_core, other_core)
    pieces = [shifted(partials[s - 1], "x", nx - s) for s in range(1, nx)]

    partial_mix, new_keys, new_values = attend(
        own_partial,
        pieces,
        scale_attn,
        gate,
        long,
        cache_logcum,
        cache_keys,
        cache_values,
        w_out,
    )

    residual = tokens.astype(F32)
    others = [shifted(partial_mix, "y", s) for s in range(1, ny)]
    mix = partial_mix.astype(F32)
    for other in others:
        mix = mix + other.astype(F32)
    mixed_res = residual + mix * inv_rms(mix) * norm_gain_mix
    col_width = width // ny
    scale_ffn = inv_rms(mixed_res)
    residual_cols = lax.dynamic_slice_in_dim(mixed_res, iy * col_width, col_width, 1)
    gain_ffn_cols = lax.dynamic_slice_in_dim(norm_gain_ffn, iy * col_width, col_width, 0)
    ffn_cols = (residual_cols * scale_ffn * gain_ffn_cols).astype(BF16)

    packed = jnp.dot(selector, ffn_cols, preferred_element_type=F32).astype(BF16)
    local_experts = EXPERTS // nz
    spread = nx // local_experts
    on_z = exchange(packed.reshape(nz, local_experts * CAP, col_width), "z")
    on_z = on_z.reshape(nz, local_experts, CAP, col_width).transpose(1, 0, 2, 3)
    on_z = on_z.reshape(local_experts, 1, 1, nz * CAP, col_width)
    outgoing = jnp.broadcast_to(on_z, (local_experts, spread, ny, nz * CAP, col_width))
    own = exchange(outgoing.reshape(nx * ny, nz * CAP, col_width), ("x", "y"))
    other = shifted(own, "c", 1)
    own_part = expert_rows(own, expert_gate, expert_up, expert_down, nx)
    other_part = expert_rows(other, expert_gate, expert_up, expert_down, nx)
    both = own_part.astype(F32) + shifted(other_part, "c", 1).astype(F32)
    summed = exchange(both.astype(BF16), ("x", "y"))
    summed = summed.reshape(local_experts, spread * ny, nz, CAP, col_width).astype(F32)
    summed = jnp.sum(summed, axis=1).astype(BF16).transpose(1, 0, 2, 3)
    returned = exchange(summed.reshape(nz, local_experts * CAP, col_width), "z")
    returned = returned.reshape(EXPERTS * CAP, col_width)
    routed = lax.dot_general(
        weighing, returned.astype(F32), (((0,), (0,)), ((), ())), preferred_element_type=F32
    )
    layer_out = (residual_cols + routed).astype(BF16)
    return (layer_out, new_keys, new_values, new_log_gate)


def solution(mesh):
    chips = Mesh(mesh.devices.reshape(8, 4, 2, 4), ("z", "x", "c", "y"))
    everyone = ("z", "x", "c", "y")
    placed = (
        P(EP, None),
        P(),
        P(EP, "y"),
        P(EP, "y"),
        P(EP, "y"),
        P(None, "y"),
        P("y"),
        P(EP, "y", None),
        P(EP, "y", None),
        P(EP, "y", None),
        P(EP),
        P("y", None),
        P(),
        P(),
        P(None, everyone),
        P(None, everyone),
        P(everyone, None),
        P(EP, None),
        P(EP, None),
    )
    return jax.shard_map(
        layer,
        mesh=chips,
        in_specs=placed,
        out_specs=(P(EP, "y"), P(EP, "y"), P(EP, "y"), P(EP, "y")),
        check_vma=False,
    )
```

```python
import functools

import jax
import jax.numpy as jnp
from jax import lax
from jax.experimental import pallas as pl
from jax.experimental.pallas import tpu as pltpu
from jax.sharding import Mesh, PartitionSpec as P


HEAD_DIM = 64
EXPERTS = 16
CAP = 8
EPSILON = 1e-06
MASKED = -1e30
EP = ("z", "x", "c")
F32 = jnp.float32
BF16 = jnp.bfloat16


def shifted(value, axis, step):
    n = lax.axis_size(axis)
    return lax.ppermute(value, axis, [(i, (i + step) % n) for i in range(n)])


def exchange(blocks, axis):
    return lax.all_to_all(blocks, axis, split_axis=0, concat_axis=0, tiled=True)


def expert_kernel(nx, rows_ref, gate_refs, up_refs, down_refs, out_ref):
    blocks, part, width = rows_ref.shape
    ny = blocks // nx
    gates, ups = [None] * len(gate_refs), [None] * len(up_refs)
    for y in range(ny):
        taken = jnp.concatenate([rows_ref[x * ny + y] for x in range(nx)], axis=0)
        deep = pl.ds(y * width, width)
        for sums, refs in ((gates, gate_refs), (ups, up_refs)):
            for k, ref in enumerate(refs):
                one = jnp.dot(taken, ref[deep, :], preferred_element_type=F32)
                sums[k] = one if sums[k] is None else sums[k] + one
    hidden = [
        (gate / (1.0 + jnp.exp(-gate)) * up).astype(BF16) for gate, up in zip(gates, ups)
    ]
    for y in range(ny):
        wide = pl.ds(y * width, width)
        back = None
        for one, ref in zip(hidden, down_refs):
            more = jnp.dot(one, ref[:, wide], preferred_element_type=F32)
            back = more if back is None else back + more
        back = back.astype(BF16)
        for x in range(nx):
            out_ref[x * ny + y] = back[x * part : (x + 1) * part]


def expert_rows(blocks, gates, ups, downs, nx):
    in_vmem = pl.BlockSpec(memory_space=pltpu.VMEM)
    count = len(gates)
    return pl.pallas_call(
        functools.partial(expert_kernel, nx),
        out_shape=jax.ShapeDtypeStruct(blocks.shape, BF16),
        in_specs=[in_vmem] + [[in_vmem] * count] * 3,
        out_specs=in_vmem,
        compiler_params=pltpu.CompilerParams(vmem_limit_bytes=20 * 2**20),
        cost_estimate=pl.CostEstimate(
            flops=2 * blocks.size * 3 * count * gates[0].shape[1],
            bytes_accessed=4 * blocks.size + 6 * count * gates[0].size,
            transcendentals=0,
        ),
    )(blocks, gates, ups, downs)


def settle_kernel(mix_refs, tokens_ref, gains_ref, selector_ref, packed_ref, cols_ref, whole_s):
    mix = None
    for ref in mix_refs:
        one = ref[...].astype(F32)
        mix = one if mix is None else mix + one
    cols = cols_ref.shape[1]
    mix = mix * lax.rsqrt(jnp.mean(mix * mix, axis=1, keepdims=True) + EPSILON)
    whole = tokens_ref[...].astype(F32) + mix * gains_ref[pl.ds(0, 1), :]
    whole_s[...] = whole
    scale = lax.rsqrt(jnp.mean(whole * whole, axis=1, keepdims=True) + EPSILON)
    here = pl.ds(pl.multiple_of(lax.axis_index("y") * cols, cols), cols)
    residual = whole_s[:, here]
    cols_ref[...] = residual
    taken = (residual * scale * gains_ref[pl.ds(1, 1), here]).astype(BF16)
    packed = jnp.dot(selector_ref[...], taken, preferred_element_type=F32)
    packed_ref[...] = packed.astype(BF16)


def settle(mixes, tokens, gains, selector, cols):
    rows, width = tokens.shape
    in_vmem = pl.BlockSpec(memory_space=pltpu.VMEM)
    return pl.pallas_call(
        settle_kernel,
        out_shape=(
            jax.ShapeDtypeStruct((selector.shape[0], cols), BF16),
            jax.ShapeDtypeStruct((rows, cols), F32),
        ),
        in_specs=[[in_vmem] * len(mixes)] + [in_vmem] * 3,
        out_specs=(in_vmem,) * 2,
        scratch_shapes=[pltpu.VMEM((rows, width), F32)],
        compiler_params=pltpu.CompilerParams(vmem_limit_bytes=6 * 2**20),
    )(mixes, tokens, gains, selector)


def fold_kernel(partials_ref, out_ref):
    nz, slots, _ = out_ref.shape
    blocks, rows, _ = partials_ref.shape
    each = rows // nz
    local_experts = slots // each
    share = blocks // local_experts
    for e in range(local_experts):
        total = partials_ref[e * share].astype(F32)
        for k in range(1, share):
            total = total + partials_ref[e * share + k].astype(F32)
        total = total.astype(BF16)
        for z in range(nz):
            out_ref[z, pl.ds(e * each, each), :] = total[z * each : (z + 1) * each]


def fold_partials(partials, local_experts, nz):
    _, rows, cols = partials.shape
    return pl.pallas_call(
        fold_kernel,
        out_shape=jax.ShapeDtypeStruct((nz, local_experts * rows // nz, cols), BF16),
        in_specs=[pl.BlockSpec(memory_space=pltpu.VMEM)],
        out_specs=pl.BlockSpec(memory_space=pltpu.VMEM),
        compiler_params=pltpu.CompilerParams(vmem_limit_bytes=6 * 2**20),
    )(partials)


def join_kernel(query_ref, key_ref, value_ref, out_ref, query_s, key_s, value_s, sems):
    parts = fetched((query_ref, key_ref, value_ref), (query_s, key_s, value_s), sems)
    joined = jnp.concatenate([part[...] for part in parts], axis=1)
    for k in range(out_ref.shape[0]):
        out_ref[k] = joined


def join(arrays, copies):
    rows = arrays[0].shape[0]
    cols = sum(array.shape[1] for array in arrays)
    return pl.pallas_call(
        join_kernel,
        out_shape=jax.ShapeDtypeStruct((copies, rows, cols), BF16),
        in_specs=[pl.BlockSpec(memory_space=pltpu.HBM)] * 3,
        out_specs=pl.BlockSpec(memory_space=pltpu.VMEM),
        scratch_shapes=places_for(arrays),
        compiler_params=pltpu.CompilerParams(vmem_limit_bytes=4 * 2**20),
    )(*in_hbm(*arrays))


def attend_kernel(
    together,
    parts,
    own_ref,
    pieces_refs,
    scale_ref,
    gate_ref,
    length_ref,
    cum_ref,
    keys_ref,
    values_ref,
    out_w_ref,
    mix_ref,
    key_ref,
    value_ref,
    q_s,
    own_s,
    weight_s,
    heads_s,
    past_s,
    cum_s,
    keys_s,
    values_s,
    out_w_s,
    sems,
):
    rows, group, head_dim = q_s.shape
    span_len = keys_ref.shape[2]
    cols = group * head_dim
    scale = HEAD_DIM ** (-0.5)
    share = rows // parts
    halves = [pl.ds(p * share, share) for p in range(parts)]

    def copies(number, source, target):
        return [
            pltpu.make_async_copy(source.at[h], target.at[h], sems.at[number, p])
            for p, h in enumerate(halves)
        ]

    key_copies = copies(0, keys_ref, keys_s)
    cum_copies = copies(1, cum_ref, cum_s)
    value_copies = copies(2, values_ref, values_s)
    out_w_copy = pltpu.make_async_copy(out_w_ref, out_w_s, sems.at[3, 0])
    for p in range(parts):
        cum_copies[p].start()
        key_copies[p].start()
    for copy in value_copies:
        copy.start()
    out_w_copy.start()

    projected = own_ref[...]
    for ref in pieces_refs:
        projected = projected + ref[...].astype(F32)
    projected = projected * scale_ref[...]
    new_key = projected[:, cols : cols + head_dim].astype(BF16)
    new_value = projected[:, cols + head_dim : cols + 2 * head_dim].astype(BF16)
    key_ref[...] = new_key
    value_ref[...] = new_value

    query = projected[:, :cols].astype(BF16).astype(F32)
    at_head = lax.broadcasted_iota(jnp.int32, (rows, group, cols), 1)
    of_head = lax.shift_right_logical(
        lax.broadcasted_iota(jnp.int32, (rows, group, cols), 2), head_dim.bit_length() - 1
    )
    on_head = at_head == of_head
    spread = jnp.where(on_head, jnp.broadcast_to(query[:, None, :], (rows, group, cols)), 0.0)
    spread = spread.reshape(rows * group, cols).astype(BF16)
    fold = (
        lax.bitwise_and(lax.broadcasted_iota(jnp.int32, (cols, head_dim), 0), head_dim - 1)
        == lax.broadcasted_iota(jnp.int32, (cols, head_dim), 1)
    )
    fold = jnp.where(fold, 1.0, 0.0).astype(BF16)
    by_head = jnp.dot(spread, fold, preferred_element_type=F32).reshape(rows, group, head_dim)
    q_s[...] = by_head
    own_s[...] = (
        jnp.sum(by_head * new_key.astype(F32)[:, None, :], axis=2, keepdims=True) * scale
    )
    places = lax.broadcasted_iota(jnp.int32, (group, span_len), 1)

    def weigh(some):
        scores = [
            jnp.dot(q_s[b].astype(BF16), keys_s[b], preferred_element_type=F32) * scale
            for b in some
        ]
        lengths = [length_ref[b] for b in some]
        cums = [cum_s[b] for b in some]
        lasts = [
            jnp.sum(jnp.where(places == n - 1, cum, 0.0), axis=1, keepdims=True)
            for n, cum in zip(lengths, cums)
        ]
        pasts = [
            jnp.where(places < n, score + ((last + gate_ref[b]) - cum), MASKED)
            for b, n, score, last, cum in zip(some, lengths, scores, lasts, cums)
        ]
        owns = [own_s[b] for b in some]
        peaks = [
            jnp.maximum(jnp.max(past, axis=1, keepdims=True), own)
            for past, own in zip(pasts, owns)
        ]
        past_exps = [jnp.exp(past - peak) for past, peak in zip(pasts, peaks)]
        own_exps = [jnp.exp(own - peak) for own, peak in zip(owns, peaks)]
        totals = [
            jnp.sum(past_exp, axis=1, keepdims=True) + own_exp
            for past_exp, own_exp in zip(past_exps, own_exps)
        ]
        for b, past_exp, own_exp, total in zip(some, past_exps, own_exps, totals):
            weight_s[b] = own_exp / total
            past_s[b] = (past_exp / total).astype(BF16)

    def mix(some):
        mixed = [
            lax.dot_general(
                past_s[b], values_s[b], (((1,), (1,)), ((), ())), preferred_element_type=F32
            )
            for b in some
        ]
        for b, one in zip(some, mixed):
            heads_s[b] = one

    for p in range(parts):
        cum_copies[p].wait()
        key_copies[p].wait()
        for first in range(p * share, (p + 1) * share, together):
            weigh(range(first, first + together))
    for p in range(parts):
        value_copies[p].wait()
        mix(range(p * share, (p + 1) * share))
    own_weight = weight_s[...].astype(BF16).astype(F32)
    heads = heads_s[...] + own_weight * new_value.astype(F32)[:, None, :]
    heads = heads.reshape(rows * group, head_dim).astype(BF16)
    wide = lax.dot_general(heads, fold, (((1,), (1,)), ((), ())), preferred_element_type=F32)
    wide = jnp.where(on_head, wide.reshape(rows, group, cols), 0.0)
    heads_out = jnp.sum(wide, axis=1).astype(BF16)
    out_w_copy.wait()
    mix_ref[...] = jnp.dot(heads_out, out_w_s[...], preferred_element_type=F32).astype(BF16)


def attend(own, pieces, scale, gate, lengths, cum, keys, values, out_w):
    rows, group, _ = cum.shape
    head_dim, width = keys.shape[1], out_w.shape[1]
    in_vmem = pl.BlockSpec(memory_space=pltpu.VMEM)
    from_hbm = pl.BlockSpec(memory_space=pltpu.HBM)
    one = jax.ShapeDtypeStruct((rows, head_dim), BF16)
    together, parts = 8, 2
    return pl.pallas_call(
        functools.partial(attend_kernel, together, parts),
        out_shape=(jax.ShapeDtypeStruct((rows, width), BF16), one, one),
        in_specs=[in_vmem, [in_vmem] * len(pieces)] + [in_vmem] * 3 + [from_hbm] * 4,
        out_specs=(in_vmem,) * 3,
        scratch_shapes=[
            pltpu.VMEM((rows, group, head_dim), F32),
            pltpu.VMEM((rows, group, 1), F32),
            pltpu.VMEM((rows, group, 1), F32),
            pltpu.VMEM((rows, group, head_dim), F32),
            pltpu.VMEM(cum.shape, BF16),
            pltpu.VMEM(cum.shape, F32),
            pltpu.VMEM(keys.shape, BF16),
            pltpu.VMEM(values.shape, BF16),
            pltpu.VMEM(out_w.shape, BF16),
            pltpu.SemaphoreType.DMA((4, parts)),
        ],
        compiler_params=pltpu.CompilerParams(vmem_limit_bytes=24 * 2**20),
        cost_estimate=pl.CostEstimate(
            flops=4 * keys.size * group + 2 * rows * out_w.size,
            bytes_accessed=4 * keys.size + 4 * cum.size + 2 * out_w.size,
            transcendentals=cum.size,
        ),
    )(own, pieces, scale, gate, lengths, *in_hbm(cum, keys, values, out_w))


def cut_kernel(nz, nx, *refs):
    outs, cut_s = refs[2 : 2 + nx], refs[2 + nx]
    tokens_ref, gain_ref = fetched(refs[:2], refs[3 + nx : -1], refs[-1])
    _, width = tokens_ref.shape
    chunk = width // (nz * nx)
    scaled = (tokens_ref[...].astype(F32) * gain_ref[...])
    for x in range(nx):
        cut_s[x] = jnp.concatenate(
            [scaled[:, (z * nx + x) * chunk : (z * nx + x + 1) * chunk] for z in range(nz)], axis=1
        )
    here = lax.axis_index("x")
    for s in range(nx):
        outs[s][...] = cut_s[lax.rem(here + s, nx)].astype(BF16)


def cut_tokens(tokens, gain, nz, nx):
    rows, width = tokens.shape
    in_vmem = pl.BlockSpec(memory_space=pltpu.VMEM)
    return pl.pallas_call(
        functools.partial(cut_kernel, nz, nx),
        out_shape=[jax.ShapeDtypeStruct((rows, width // nx), BF16)] * nx,
        in_specs=[pl.BlockSpec(memory_space=pltpu.HBM)] * 2,
        out_specs=[in_vmem] * nx,
        scratch_shapes=[pltpu.VMEM((nx, rows, width // nx), F32)] + places_for((tokens, gain)),
        compiler_params=pltpu.CompilerParams(vmem_limit_bytes=4 * 2**20),
    )(*in_hbm(tokens, gain))


def multiply_kernel(count, *refs):
    token_refs, (same_ref, other_ref), outs = refs[:count], refs[count : count + 2], refs[count + 2 :]
    first = lax.axis_index("c") == 0
    same, other = same_ref[...], other_ref[...]
    weights = jnp.concatenate(
        (jnp.where(first, same, other), jnp.where(first, other, same)), axis=1
    )
    weights = weights.reshape(-1, weights.shape[-1])
    tokens = jnp.concatenate([ref[...] for ref in token_refs], axis=0)
    product = jnp.dot(tokens, weights, preferred_element_type=F32)
    rows = token_refs[0].shape[0]
    for s, out in enumerate(outs):
        out[...] = product[s * rows : (s + 1) * rows].astype(out.dtype)


def multiply(pieces, same, other):
    rows = pieces[0].shape[0]
    cols = same.shape[2]
    in_vmem = pl.BlockSpec(memory_space=pltpu.VMEM)
    kinds = [F32] + [BF16] * (len(pieces) - 1)
    return pl.pallas_call(
        functools.partial(multiply_kernel, len(pieces)),
        out_shape=[jax.ShapeDtypeStruct((rows, cols), kind) for kind in kinds],
        in_specs=[in_vmem] * (len(pieces) + 2),
        out_specs=[in_vmem] * len(pieces),
        compiler_params=pltpu.CompilerParams(vmem_limit_bytes=8 * 2**20),
        cost_estimate=pl.CostEstimate(
            flops=4 * rows * len(pieces) * same.size,
            bytes_accessed=4 * same.size,
            transcendentals=0,
        ),
    )(*pieces, same, other)


def fetched(sources, targets, sems):
    copies = [
        pltpu.make_async_copy(source, target, sems.at[k])
        for k, (source, target) in enumerate(zip(sources, targets))
    ]
    for copy in copies:
        copy.start()
    for copy in copies:
        copy.wait()
    return targets


def in_hbm(*arrays):
    return [pltpu.with_memory_space_constraint(array, pltpu.HBM) for array in arrays]


def places_for(arrays):
    return [pltpu.VMEM(array.shape, array.dtype) for array in arrays] + [
        pltpu.SemaphoreType.DMA((len(arrays),))
    ]


def early_kernel(count, *refs):
    (
        scale_ref,
        log_gate_ref,
        gate_ref,
        long_ref,
        selector_ref,
        weighing_ref,
        kept_ref,
        gains_ref,
    ) = refs[count : count + 8]
    (
        tokens_ref,
        gain_ref,
        gain_mix_ref,
        gain_ffn_ref,
        forget_ref,
        bias_ref,
        length_ref,
        routes_ref,
        weights_ref,
    ) = fetched(refs[:count], refs[count + 8 : -1], refs[-1])
    kept_ref[...] = tokens_ref[...]
    gains_ref[pl.ds(0, 1), :] = gain_mix_ref[...]
    gains_ref[pl.ds(1, 1), :] = gain_ffn_ref[...]

    tokens = tokens_ref[...].astype(F32)
    rows = tokens.shape[0]
    group = forget_ref.shape[0]
    scale = lax.rsqrt(jnp.mean(tokens * tokens, axis=1, keepdims=True) + EPSILON)
    scale_ref[...] = scale
    normed = (tokens * scale * gain_ref[...]).astype(BF16)
    logits = lax.dot_general(
        normed, forget_ref[...], (((1,), (1,)), ((), ())), preferred_element_type=F32
    )
    logits = logits + bias_ref[...]
    gate = jnp.minimum(logits, 0.0) - jnp.log1p(jnp.exp(-jnp.abs(logits)))
    log_gate_ref[...] = gate
    same = lax.broadcasted_iota(jnp.int32, (rows, group, group), 1) == lax.broadcasted_iota(
        jnp.int32, (rows, group, group), 2
    )
    gate_ref[...] = jnp.sum(jnp.where(same, gate[:, None, :], 0.0), axis=2, keepdims=True)
    mine = lax.broadcasted_iota(jnp.int32, (rows, rows), 0) == lax.broadcasted_iota(
        jnp.int32, (rows, rows), 1
    )
    lengths = jnp.where(mine, length_ref[...].astype(F32), 0.0)
    lengths = jnp.sum(lengths, axis=1, keepdims=True)
    long_ref[...] = jnp.broadcast_to(lengths[:, None, :], long_ref.shape).astype(jnp.int32)

    top = routes_ref.shape[0]
    named = [routes_ref[pl.ds(k, 1), :] for k in range(top)]
    experts = lax.broadcasted_iota(jnp.int32, (EXPERTS, rows), 0)
    hits = [jnp.where(experts == one, 1.0, 0.0) for one in named]
    both = sum(hits[1:], hits[0])
    before = lax.broadcasted_iota(jnp.int32, (rows, rows), 0) < lax.broadcasted_iota(
        jnp.int32, (rows, rows), 1
    )
    earlier = jnp.dot(
        both.astype(BF16), jnp.where(before, 1.0, 0.0).astype(BF16), preferred_element_type=F32
    )
    places = lax.broadcasted_iota(jnp.int32, (EXPERTS * CAP, rows), 0)
    chosen = jnp.zeros((EXPERTS * CAP, rows), F32)
    weighed = jnp.zeros((EXPERTS * CAP, rows), F32)
    for k in range(top):
        slot = jnp.sum(earlier * hits[k], axis=0, keepdims=True).astype(jnp.int32)
        there = jnp.where(places == named[k] * CAP + slot, 1.0, 0.0)
        chosen = chosen + there
        weighed = weighed + there * weights_ref[pl.ds(k, 1), :]
    selector_ref[...] = chosen.astype(BF16)
    weighing_ref[...] = weighed


def early(*arrays):
    in_vmem = pl.BlockSpec(memory_space=pltpu.VMEM)
    tokens, _, _, _, forget, *_ = arrays
    rows, group = tokens.shape[0], forget.shape[0]
    slots = EXPERTS * CAP
    return pl.pallas_call(
        functools.partial(early_kernel, len(arrays)),
        out_shape=(
            jax.ShapeDtypeStruct((rows, 1), F32),
            jax.ShapeDtypeStruct((rows, group), F32),
            jax.ShapeDtypeStruct((rows, group, 1), F32),
            jax.ShapeDtypeStruct((rows, group, 1), jnp.int32),
            jax.ShapeDtypeStruct((slots, rows), BF16),
            jax.ShapeDtypeStruct((slots, rows), F32),
            jax.ShapeDtypeStruct(tokens.shape, BF16),
            jax.ShapeDtypeStruct((2, tokens.shape[1]), F32),
        ),
        in_specs=[pl.BlockSpec(memory_space=pltpu.HBM)] * len(arrays),
        out_specs=(in_vmem,) * 8,
        scratch_shapes=places_for(arrays),
        compiler_params=pltpu.CompilerParams(vmem_limit_bytes=6 * 2**20),
    )(*in_hbm(*arrays))


def layer(
    tokens,
    norm_gain_attn,
    w_query,
    w_key,
    w_value,
    w_forget,
    forget_bias,
    cache_keys,
    cache_values,
    cache_logcum,
    lengths,
    w_out,
    norm_gain_mix,
    norm_gain_ffn,
    expert_gate,
    expert_up,
    expert_down,
    routes,
    route_weights,
):
    _, width = tokens.shape
    nz, nx, _, ny = (lax.axis_size(a) for a in ("z", "x", "c", "y"))

    scale_attn, new_log_gate, gate, long, selector, weighing, kept, gains = early(
        tokens,
        norm_gain_attn.reshape(1, width),
        norm_gain_mix.reshape(1, width),
        norm_gain_ffn.reshape(1, width),
        w_forget.T,
        forget_bias.reshape(1, -1),
        lengths.reshape(1, -1),
        routes.T,
        route_weights.T,
    )

    weights = join((w_query, w_key, w_value), nz)
    same_core = exchange(weights, "z")
    others = [shifted(w, "c", 1) for w in (expert_gate, expert_up, expert_down)]
    other_core = shifted(same_core, "c", 1)
    mine = cut_tokens(tokens, norm_gain_attn.reshape(1, width), nz, nx)
    moved = [shifted(mine[s], "x", s) for s in range(1, nx)]
    own_partial, *partials = multiply([mine[0]] + moved, same_core, other_core)
    pieces = [shifted(partials[s - 1], "x", nx - s) for s in range(1, nx)]

    partial_mix, new_keys, new_values = attend(
        own_partial,
        pieces,
        scale_attn,
        gate,
        long,
        cache_logcum,
        cache_keys,
        cache_values,
        w_out,
    )

    mixes = [partial_mix] + [shifted(partial_mix, "y", s) for s in range(1, ny)]
    col_width = width // ny
    packed, residual_cols = settle(mixes, kept, gains, selector, col_width)

    local_experts = EXPERTS // nz
    spread = nx // local_experts
    on_z = exchange(packed.reshape(nz, local_experts * CAP, col_width), "z")
    on_z = on_z.reshape(nz, local_experts, CAP, col_width).transpose(1, 0, 2, 3)
    on_z = on_z.reshape(local_experts, 1, 1, nz * CAP, col_width)
    outgoing = jnp.broadcast_to(on_z, (local_experts, spread, ny, nz * CAP, col_width))
    own = exchange(outgoing.reshape(nx * ny, nz * CAP, col_width), ("x", "y"))
    part = expert_rows(own, *[list(p) for p in zip((expert_gate, expert_up, expert_down), others)], nx)
    summed = exchange(part, ("x", "y"))
    returned = exchange(fold_partials(summed, local_experts, nz), "z")
    returned = returned.reshape(EXPERTS * CAP, col_width)
    routed = lax.dot_general(
        weighing, returned.astype(F32), (((0,), (0,)), ((), ())), preferred_element_type=F32
    )
    layer_out = (residual_cols + routed).astype(BF16)
    return (layer_out, new_keys, new_values, new_log_gate)


def solution(mesh):
    chips = Mesh(mesh.devices.reshape(8, 4, 2, 4), ("z", "x", "c", "y"))
    everyone = ("z", "x", "c", "y")
    placed = (
        P(EP, None),
        P(),
        P(EP, "y"),
        P(EP, "y"),
        P(EP, "y"),
        P(None, "y"),
        P("y"),
        P(EP, "y", None),
        P(EP, "y", None),
        P(EP, "y", None),
        P(EP),
        P("y", None),
        P(),
        P(),
        P(None, everyone),
        P(None, everyone),
        P(everyone, None),
        P(EP, None),
        P(EP, None),
    )
    return jax.shard_map(
        layer,
        mesh=chips,
        in_specs=placed,
        out_specs=(P(EP, "y"), P(EP, "y"), P(EP, "y"), P(EP, "y")),
        check_vma=False,
    )
```

```python
import functools

import jax
import jax.numpy as jnp
from jax import lax
from jax.experimental import pallas as pl
from jax.experimental.pallas import tpu as pltpu
from jax.sharding import Mesh, PartitionSpec as P


HEAD_DIM = 64
EXPERTS = 16
CAP = 8
EPSILON = 1e-06
MASKED = -1e30
EP = ("z", "x", "c")
F32 = jnp.float32
BF16 = jnp.bfloat16


def shifted(value, axis, step):
    n = lax.axis_size(axis)
    return lax.ppermute(value, axis, [(i, (i + step) % n) for i in range(n)])


def exchange(blocks, axis):
    return lax.all_to_all(blocks, axis, split_axis=0, concat_axis=0, tiled=True)


def expert_kernel(nx, rows_ref, gate_refs, up_refs, down_refs, out_ref):
    blocks, part, width = rows_ref.shape
    ny = blocks // nx
    gates, ups = [None] * len(gate_refs), [None] * len(up_refs)
    for y in range(ny):
        taken = jnp.concatenate([rows_ref[x * ny + y] for x in range(nx)], axis=0)
        deep = pl.ds(y * width, width)
        for sums, refs in ((gates, gate_refs), (ups, up_refs)):
            for k, ref in enumerate(refs):
                one = jnp.dot(taken, ref[deep, :], preferred_element_type=F32)
                sums[k] = one if sums[k] is None else sums[k] + one
    hidden = [
        (gate / (1.0 + jnp.exp(-gate)) * up).astype(BF16) for gate, up in zip(gates, ups)
    ]
    for y in range(ny):
        wide = pl.ds(y * width, width)
        back = None
        for one, ref in zip(hidden, down_refs):
            more = jnp.dot(one, ref[:, wide], preferred_element_type=F32)
            back = more if back is None else back + more
        back = back.astype(BF16)
        for x in range(nx):
            out_ref[x * ny + y] = back[x * part : (x + 1) * part]


def expert_rows(blocks, gates, ups, downs, nx):
    in_vmem = pl.BlockSpec(memory_space=pltpu.VMEM)
    count = len(gates)
    return pl.pallas_call(
        functools.partial(expert_kernel, nx),
        out_shape=jax.ShapeDtypeStruct(blocks.shape, BF16),
        in_specs=[in_vmem] + [[in_vmem] * count] * 3,
        out_specs=in_vmem,
        compiler_params=pltpu.CompilerParams(vmem_limit_bytes=20 * 2**20),
        cost_estimate=pl.CostEstimate(
            flops=2 * blocks.size * 3 * count * gates[0].shape[1],
            bytes_accessed=4 * blocks.size + 6 * count * gates[0].size,
            transcendentals=0,
        ),
    )(blocks, gates, ups, downs)


def settle_kernel(mix_refs, tokens_ref, gains_ref, selector_ref, packed_ref, cols_ref, whole_s):
    mix = None
    for ref in mix_refs:
        one = ref[...].astype(F32)
        mix = one if mix is None else mix + one
    cols = cols_ref.shape[1]
    mix = mix * lax.rsqrt(jnp.mean(mix * mix, axis=1, keepdims=True) + EPSILON)
    whole = tokens_ref[...].astype(F32) + mix * gains_ref[pl.ds(0, 1), :]
    whole_s[...] = whole
    scale = lax.rsqrt(jnp.mean(whole * whole, axis=1, keepdims=True) + EPSILON)
    here = pl.ds(pl.multiple_of(lax.axis_index("y") * cols, cols), cols)
    residual = whole_s[:, here]
    cols_ref[...] = residual
    taken = (residual * scale * gains_ref[pl.ds(1, 1), here]).astype(BF16)
    packed = jnp.dot(selector_ref[...], taken, preferred_element_type=F32)
    packed_ref[...] = packed.astype(BF16)


def settle(mixes, tokens, gains, selector, cols):
    rows, width = tokens.shape
    in_vmem = pl.BlockSpec(memory_space=pltpu.VMEM)
    return pl.pallas_call(
        settle_kernel,
        out_shape=(
            jax.ShapeDtypeStruct((selector.shape[0], cols), BF16),
            jax.ShapeDtypeStruct((rows, cols), F32),
        ),
        in_specs=[[in_vmem] * len(mixes)] + [in_vmem] * 3,
        out_specs=(in_vmem,) * 2,
        scratch_shapes=[pltpu.VMEM((rows, width), F32)],
        compiler_params=pltpu.CompilerParams(vmem_limit_bytes=6 * 2**20),
    )(mixes, tokens, gains, selector)


def fold_kernel(partials_ref, out_ref):
    nz, slots, _ = out_ref.shape
    blocks, rows, _ = partials_ref.shape
    each = rows // nz
    local_experts = slots // each
    share = blocks // local_experts
    for e in range(local_experts):
        total = partials_ref[e * share].astype(F32)
        for k in range(1, share):
            total = total + partials_ref[e * share + k].astype(F32)
        total = total.astype(BF16)
        for z in range(nz):
            out_ref[z, pl.ds(e * each, each), :] = total[z * each : (z + 1) * each]


def fold_partials(partials, local_experts, nz):
    _, rows, cols = partials.shape
    return pl.pallas_call(
        fold_kernel,
        out_shape=jax.ShapeDtypeStruct((nz, local_experts * rows // nz, cols), BF16),
        in_specs=[pl.BlockSpec(memory_space=pltpu.VMEM)],
        out_specs=pl.BlockSpec(memory_space=pltpu.VMEM),
        compiler_params=pltpu.CompilerParams(vmem_limit_bytes=6 * 2**20),
    )(partials)


def join_kernel(query_ref, key_ref, value_ref, out_ref, query_s, key_s, value_s, sems):
    parts = fetched((query_ref, key_ref, value_ref), (query_s, key_s, value_s), sems)
    joined = jnp.concatenate([part[...] for part in parts], axis=1)
    for k in range(out_ref.shape[0]):
        out_ref[k] = joined


def join(arrays, copies):
    rows = arrays[0].shape[0]
    cols = sum(array.shape[1] for array in arrays)
    return pl.pallas_call(
        join_kernel,
        out_shape=jax.ShapeDtypeStruct((copies, rows, cols), BF16),
        in_specs=[pl.BlockSpec(memory_space=pltpu.HBM)] * 3,
        out_specs=pl.BlockSpec(memory_space=pltpu.VMEM),
        scratch_shapes=places_for(arrays),
        compiler_params=pltpu.CompilerParams(vmem_limit_bytes=4 * 2**20),
    )(*in_hbm(*arrays))


def attend_kernel(
    together,
    parts,
    own_ref,
    pieces_refs,
    scale_ref,
    gate_ref,
    length_ref,
    cum_ref,
    keys_ref,
    values_ref,
    out_w_ref,
    mix_ref,
    key_ref,
    value_ref,
    q_s,
    own_s,
    weight_s,
    heads_s,
    past_s,
    keys_s,
    values_s,
    sems,
):
    rows, group, head_dim = q_s.shape
    span_len = keys_ref.shape[2]
    cols = group * head_dim
    scale = HEAD_DIM ** (-0.5)
    share = rows // parts
    halves = [pl.ds(p * share, share) for p in range(parts)]

    def copies(number, source, target):
        return [
            pltpu.make_async_copy(source.at[h], target.at[h], sems.at[number, p])
            for p, h in enumerate(halves)
        ]

    key_copies = copies(0, keys_ref, keys_s)
    value_copies = copies(1, values_ref, values_s)
    for copy in key_copies + value_copies:
        copy.start()

    projected = own_ref[...]
    for ref in pieces_refs:
        projected = projected + ref[...].astype(F32)
    projected = projected * scale_ref[...]
    new_key = projected[:, cols : cols + head_dim].astype(BF16)
    new_value = projected[:, cols + head_dim : cols + 2 * head_dim].astype(BF16)
    key_ref[...] = new_key
    value_ref[...] = new_value

    query = projected[:, :cols].astype(BF16).astype(F32)
    at_head = lax.broadcasted_iota(jnp.int32, (rows, group, cols), 1)
    of_head = lax.shift_right_logical(
        lax.broadcasted_iota(jnp.int32, (rows, group, cols), 2), head_dim.bit_length() - 1
    )
    on_head = at_head == of_head
    spread = jnp.where(on_head, jnp.broadcast_to(query[:, None, :], (rows, group, cols)), 0.0)
    spread = spread.reshape(rows * group, cols).astype(BF16)
    fold = (
        lax.bitwise_and(lax.broadcasted_iota(jnp.int32, (cols, head_dim), 0), head_dim - 1)
        == lax.broadcasted_iota(jnp.int32, (cols, head_dim), 1)
    )
    fold = jnp.where(fold, 1.0, 0.0).astype(BF16)
    by_head = jnp.dot(spread, fold, preferred_element_type=F32).reshape(rows, group, head_dim)
    q_s[...] = by_head
    own_s[...] = (
        jnp.sum(by_head * new_key.astype(F32)[:, None, :], axis=2, keepdims=True) * scale
    )
    places = lax.broadcasted_iota(jnp.int32, (group, span_len), 1)

    def weigh(some):
        scores = [
            jnp.dot(q_s[b].astype(BF16), keys_s[b], preferred_element_type=F32) * scale
            for b in some
        ]
        lengths = [length_ref[b] for b in some]
        cums = [cum_ref[b] for b in some]
        lasts = [
            jnp.sum(jnp.where(places == n - 1, cum, 0.0), axis=1, keepdims=True)
            for n, cum in zip(lengths, cums)
        ]
        pasts = [
            jnp.where(places < n, score + ((last + gate_ref[b]) - cum), MASKED)
            for b, n, score, last, cum in zip(some, lengths, scores, lasts, cums)
        ]
        owns = [own_s[b] for b in some]
        peaks = [
            jnp.maximum(jnp.max(past, axis=1, keepdims=True), own)
            for past, own in zip(pasts, owns)
        ]
        past_exps = [jnp.exp(past - peak) for past, peak in zip(pasts, peaks)]
        own_exps = [jnp.exp(own - peak) for own, peak in zip(owns, peaks)]
        totals = [
            jnp.sum(past_exp, axis=1, keepdims=True) + own_exp
            for past_exp, own_exp in zip(past_exps, own_exps)
        ]
        for b, past_exp, own_exp, total in zip(some, past_exps, own_exps, totals):
            weight_s[b] = own_exp / total
            past_s[b] = (past_exp / total).astype(BF16)

    def mix(some):
        mixed = [
            lax.dot_general(
                past_s[b], values_s[b], (((1,), (1,)), ((), ())), preferred_element_type=F32
            )
            for b in some
        ]
        for b, one in zip(some, mixed):
            heads_s[b] = one

    for p in range(parts):
        key_copies[p].wait()
        for first in range(p * share, (p + 1) * share, together):
            weigh(range(first, first + together))
    for p in range(parts):
        value_copies[p].wait()
        mix(range(p * share, (p + 1) * share))
    own_weight = weight_s[...].astype(BF16).astype(F32)
    heads = heads_s[...] + own_weight * new_value.astype(F32)[:, None, :]
    heads = heads.reshape(rows * group, head_dim).astype(BF16)
    wide = lax.dot_general(heads, fold, (((1,), (1,)), ((), ())), preferred_element_type=F32)
    wide = jnp.where(on_head, wide.reshape(rows, group, cols), 0.0)
    heads_out = jnp.sum(wide, axis=1).astype(BF16)
    mix_ref[...] = jnp.dot(heads_out, out_w_ref[...], preferred_element_type=F32).astype(BF16)


def load_kernel(count, *refs):
    fetched(refs[:count], refs[count:-1], refs[-1])


def load(*arrays):
    return pl.pallas_call(
        functools.partial(load_kernel, len(arrays)),
        out_shape=[jax.ShapeDtypeStruct(array.shape, array.dtype) for array in arrays],
        in_specs=[pl.BlockSpec(memory_space=pltpu.HBM)] * len(arrays),
        out_specs=[pl.BlockSpec(memory_space=pltpu.VMEM)] * len(arrays),
        scratch_shapes=[pltpu.SemaphoreType.DMA((len(arrays),))],
        compiler_params=pltpu.CompilerParams(vmem_limit_bytes=8 * 2**20),
    )(*in_hbm(*arrays))


def attend(own, pieces, scale, gate, lengths, cum, keys, values, out_w):
    rows, group, _ = cum.shape
    head_dim, width = keys.shape[1], out_w.shape[1]
    in_vmem = pl.BlockSpec(memory_space=pltpu.VMEM)
    from_hbm = pl.BlockSpec(memory_space=pltpu.HBM)
    one = jax.ShapeDtypeStruct((rows, head_dim), BF16)
    together, parts = 8, 2
    return pl.pallas_call(
        functools.partial(attend_kernel, together, parts),
        out_shape=(jax.ShapeDtypeStruct((rows, width), BF16), one, one),
        in_specs=[in_vmem, [in_vmem] * len(pieces)]
        + [in_vmem] * 4
        + [from_hbm] * 2
        + [in_vmem],
        out_specs=(in_vmem,) * 3,
        scratch_shapes=[
            pltpu.VMEM((rows, group, head_dim), F32),
            pltpu.VMEM((rows, group, 1), F32),
            pltpu.VMEM((rows, group, 1), F32),
            pltpu.VMEM((rows, group, head_dim), F32),
            pltpu.VMEM(cum.shape, BF16),
            pltpu.VMEM(keys.shape, BF16),
            pltpu.VMEM(values.shape, BF16),
            pltpu.SemaphoreType.DMA((2, parts)),
        ],
        compiler_params=pltpu.CompilerParams(vmem_limit_bytes=24 * 2**20),
        cost_estimate=pl.CostEstimate(
            flops=4 * keys.size * group + 2 * rows * out_w.size,
            bytes_accessed=4 * keys.size + 4 * cum.size + 2 * out_w.size,
            transcendentals=cum.size,
        ),
    )(own, pieces, scale, gate, lengths, cum, *in_hbm(keys, values), out_w)


def cut_kernel(nz, nx, *refs):
    outs, cut_s = refs[2 : 2 + nx], refs[2 + nx]
    tokens_ref, gain_ref = fetched(refs[:2], refs[3 + nx : -1], refs[-1])
    _, width = tokens_ref.shape
    chunk = width // (nz * nx)
    scaled = (tokens_ref[...].astype(F32) * gain_ref[...])
    for x in range(nx):
        cut_s[x] = jnp.concatenate(
            [scaled[:, (z * nx + x) * chunk : (z * nx + x + 1) * chunk] for z in range(nz)], axis=1
        )
    here = lax.axis_index("x")
    for s in range(nx):
        outs[s][...] = cut_s[lax.rem(here + s, nx)].astype(BF16)


def cut_tokens(tokens, gain, nz, nx):
    rows, width = tokens.shape
    in_vmem = pl.BlockSpec(memory_space=pltpu.VMEM)
    return pl.pallas_call(
        functools.partial(cut_kernel, nz, nx),
        out_shape=[jax.ShapeDtypeStruct((rows, width // nx), BF16)] * nx,
        in_specs=[pl.BlockSpec(memory_space=pltpu.HBM)] * 2,
        out_specs=[in_vmem] * nx,
        scratch_shapes=[pltpu.VMEM((nx, rows, width // nx), F32)] + places_for((tokens, gain)),
        compiler_params=pltpu.CompilerParams(vmem_limit_bytes=4 * 2**20),
    )(*in_hbm(tokens, gain))


def multiply_kernel(count, *refs):
    token_refs, (same_ref, other_ref), outs = refs[:count], refs[count : count + 2], refs[count + 2 :]
    first = lax.axis_index("c") == 0
    same, other = same_ref[...], other_ref[...]
    weights = jnp.concatenate(
        (jnp.where(first, same, other), jnp.where(first, other, same)), axis=1
    )
    weights = weights.reshape(-1, weights.shape[-1])
    tokens = jnp.concatenate([ref[...] for ref in token_refs], axis=0)
    product = jnp.dot(tokens, weights, preferred_element_type=F32)
    rows = token_refs[0].shape[0]
    for s, out in enumerate(outs):
        out[...] = product[s * rows : (s + 1) * rows].astype(out.dtype)


def multiply(pieces, same, other):
    rows = pieces[0].shape[0]
    cols = same.shape[2]
    in_vmem = pl.BlockSpec(memory_space=pltpu.VMEM)
    kinds = [F32] + [BF16] * (len(pieces) - 1)
    return pl.pallas_call(
        functools.partial(multiply_kernel, len(pieces)),
        out_shape=[jax.ShapeDtypeStruct((rows, cols), kind) for kind in kinds],
        in_specs=[in_vmem] * (len(pieces) + 2),
        out_specs=[in_vmem] * len(pieces),
        compiler_params=pltpu.CompilerParams(vmem_limit_bytes=8 * 2**20),
        cost_estimate=pl.CostEstimate(
            flops=4 * rows * len(pieces) * same.size,
            bytes_accessed=4 * same.size,
            transcendentals=0,
        ),
    )(*pieces, same, other)


def fetched(sources, targets, sems):
    copies = [
        pltpu.make_async_copy(source, target, sems.at[k])
        for k, (source, target) in enumerate(zip(sources, targets))
    ]
    for copy in copies:
        copy.start()
    for copy in copies:
        copy.wait()
    return targets


def in_hbm(*arrays):
    return [pltpu.with_memory_space_constraint(array, pltpu.HBM) for array in arrays]


def places_for(arrays):
    return [pltpu.VMEM(array.shape, array.dtype) for array in arrays] + [
        pltpu.SemaphoreType.DMA((len(arrays),))
    ]


def early_kernel(count, *refs):
    (
        scale_ref,
        log_gate_ref,
        gate_ref,
        long_ref,
        selector_ref,
        weighing_ref,
        kept_ref,
        gains_ref,
    ) = refs[count : count + 8]
    (
        tokens_ref,
        gain_ref,
        gain_mix_ref,
        gain_ffn_ref,
        forget_ref,
        bias_ref,
        length_ref,
        routes_ref,
        weights_ref,
    ) = fetched(refs[:count], refs[count + 8 : -1], refs[-1])
    kept_ref[...] = tokens_ref[...]
    gains_ref[pl.ds(0, 1), :] = gain_mix_ref[...]
    gains_ref[pl.ds(1, 1), :] = gain_ffn_ref[...]

    tokens = tokens_ref[...].astype(F32)
    rows = tokens.shape[0]
    group = forget_ref.shape[0]
    scale = lax.rsqrt(jnp.mean(tokens * tokens, axis=1, keepdims=True) + EPSILON)
    scale_ref[...] = scale
    normed = (tokens * scale * gain_ref[...]).astype(BF16)
    logits = lax.dot_general(
        normed, forget_ref[...], (((1,), (1,)), ((), ())), preferred_element_type=F32
    )
    logits = logits + bias_ref[...]
    gate = jnp.minimum(logits, 0.0) - jnp.log1p(jnp.exp(-jnp.abs(logits)))
    across = lax.dot_general(
        forget_ref[...], normed, (((1,), (1,)), ((), ())), preferred_element_type=F32
    )
    one = lax.broadcasted_iota(jnp.int32, (group, group), 0) == lax.broadcasted_iota(
        jnp.int32, (group, group), 1
    )
    across = across + jnp.sum(jnp.where(one, bias_ref[...], 0.0), axis=1, keepdims=True)
    log_gate_ref[...] = jnp.minimum(across, 0.0) - jnp.log1p(jnp.exp(-jnp.abs(across)))
    same = lax.broadcasted_iota(jnp.int32, (rows, group, group), 1) == lax.broadcasted_iota(
        jnp.int32, (rows, group, group), 2
    )
    gate_ref[...] = jnp.sum(jnp.where(same, gate[:, None, :], 0.0), axis=2, keepdims=True)
    mine = lax.broadcasted_iota(jnp.int32, (rows, rows), 0) == lax.broadcasted_iota(
        jnp.int32, (rows, rows), 1
    )
    lengths = jnp.where(mine, length_ref[...].astype(F32), 0.0)
    lengths = jnp.sum(lengths, axis=1, keepdims=True)
    long_ref[...] = jnp.broadcast_to(lengths[:, None, :], long_ref.shape).astype(jnp.int32)

    top = routes_ref.shape[0]
    named = [routes_ref[pl.ds(k, 1), :] for k in range(top)]
    experts = lax.broadcasted_iota(jnp.int32, (EXPERTS, rows), 0)
    hits = [jnp.where(experts == one, 1.0, 0.0) for one in named]
    both = sum(hits[1:], hits[0])
    before = lax.broadcasted_iota(jnp.int32, (rows, rows), 0) < lax.broadcasted_iota(
        jnp.int32, (rows, rows), 1
    )
    earlier = jnp.dot(
        both.astype(BF16), jnp.where(before, 1.0, 0.0).astype(BF16), preferred_element_type=F32
    )
    places = lax.broadcasted_iota(jnp.int32, (EXPERTS * CAP, rows), 0)
    chosen = jnp.zeros((EXPERTS * CAP, rows), F32)
    weighed = jnp.zeros((EXPERTS * CAP, rows), F32)
    for k in range(top):
        slot = jnp.sum(earlier * hits[k], axis=0, keepdims=True).astype(jnp.int32)
        there = jnp.where(places == named[k] * CAP + slot, 1.0, 0.0)
        chosen = chosen + there
        weighed = weighed + there * weights_ref[pl.ds(k, 1), :]
    selector_ref[...] = chosen.astype(BF16)
    weighing_ref[...] = weighed


def early(*arrays):
    in_vmem = pl.BlockSpec(memory_space=pltpu.VMEM)
    tokens, _, _, _, forget, *_ = arrays
    rows, group = tokens.shape[0], forget.shape[0]
    slots = EXPERTS * CAP
    return pl.pallas_call(
        functools.partial(early_kernel, len(arrays)),
        out_shape=(
            jax.ShapeDtypeStruct((rows, 1), F32),
            jax.ShapeDtypeStruct((group, rows), F32),
            jax.ShapeDtypeStruct((rows, group, 1), F32),
            jax.ShapeDtypeStruct((rows, group, 1), jnp.int32),
            jax.ShapeDtypeStruct((slots, rows), BF16),
            jax.ShapeDtypeStruct((slots, rows), F32),
            jax.ShapeDtypeStruct(tokens.shape, BF16),
            jax.ShapeDtypeStruct((2, tokens.shape[1]), F32),
        ),
        in_specs=[pl.BlockSpec(memory_space=pltpu.HBM)] * len(arrays),
        out_specs=(in_vmem,) * 8,
        scratch_shapes=places_for(arrays),
        compiler_params=pltpu.CompilerParams(vmem_limit_bytes=6 * 2**20),
    )(*in_hbm(*arrays))


def layer(
    tokens,
    norm_gain_attn,
    w_query,
    w_key,
    w_value,
    w_forget,
    forget_bias,
    cache_keys,
    cache_values,
    cache_logcum,
    lengths,
    w_out,
    norm_gain_mix,
    norm_gain_ffn,
    expert_gate,
    expert_up,
    expert_down,
    routes,
    route_weights,
):
    _, width = tokens.shape
    nz, nx, _, ny = (lax.axis_size(a) for a in ("z", "x", "c", "y"))

    scale_attn, new_log_gate, gate, long, selector, weighing, kept, gains = early(
        tokens,
        norm_gain_attn.reshape(1, width),
        norm_gain_mix.reshape(1, width),
        norm_gain_ffn.reshape(1, width),
        w_forget.T,
        forget_bias.reshape(1, -1),
        lengths.reshape(1, -1),
        routes.T,
        route_weights.T,
    )

    weights = join((w_query, w_key, w_value), nz)
    same_core = exchange(weights, "z")
    others = [shifted(w, "c", 1) for w in (expert_gate, expert_up, expert_down)]
    other_core = shifted(same_core, "c", 1)
    mine = cut_tokens(tokens, norm_gain_attn.reshape(1, width), nz, nx)
    moved = [shifted(mine[s], "x", s) for s in range(1, nx)]
    own_partial, *partials = multiply([mine[0]] + moved, same_core, other_core)
    pieces = [shifted(partials[s - 1], "x", nx - s) for s in range(1, nx)]

    logcum, out_rows = load(cache_logcum, w_out)

    partial_mix, new_keys, new_values = attend(
        own_partial,
        pieces,
        scale_attn,
        gate,
        long,
        logcum,
        cache_keys,
        cache_values,
        out_rows,
    )

    mixes = [partial_mix] + [shifted(partial_mix, "y", s) for s in range(1, ny)]
    col_width = width // ny
    packed, residual_cols = settle(mixes, kept, gains, selector, col_width)

    local_experts = EXPERTS // nz
    spread = nx // local_experts
    on_z = exchange(packed.reshape(nz, local_experts * CAP, col_width), "z")
    on_z = on_z.reshape(nz, local_experts, CAP, col_width).transpose(1, 0, 2, 3)
    on_z = on_z.reshape(local_experts, 1, 1, nz * CAP, col_width)
    outgoing = jnp.broadcast_to(on_z, (local_experts, spread, ny, nz * CAP, col_width))
    own = exchange(outgoing.reshape(nx * ny, nz * CAP, col_width), ("x", "y"))
    part = expert_rows(own, *[list(p) for p in zip((expert_gate, expert_up, expert_down), others)], nx)
    summed = exchange(part, ("x", "y"))
    returned = exchange(fold_partials(summed, local_experts, nz), "z")
    returned = returned.reshape(EXPERTS * CAP, col_width)
    routed = lax.dot_general(
        weighing, returned.astype(F32), (((0,), (0,)), ((), ())), preferred_element_type=F32
    )
    layer_out = (residual_cols + routed).astype(BF16)
    return (layer_out, new_keys, new_values, new_log_gate.T)


def solution(mesh):
    chips = Mesh(mesh.devices.reshape(8, 4, 2, 4), ("z", "x", "c", "y"))
    everyone = ("z", "x", "c", "y")
    placed = (
        P(EP, None),
        P(),
        P(EP, "y"),
        P(EP, "y"),
        P(EP, "y"),
        P(None, "y"),
        P("y"),
        P(EP, "y", None),
        P(EP, "y", None),
        P(EP, "y", None),
        P(EP),
        P("y", None),
        P(),
        P(),
        P(None, everyone),
        P(None, everyone),
        P(everyone, None),
        P(EP, None),
        P(EP, None),
    )
    return jax.shard_map(
        layer,
        mesh=chips,
        in_specs=placed,
        out_specs=(P(EP, "y"), P(EP, "y"), P(EP, "y"), P(EP, "y")),
        check_vma=False,
    )
```

```python
import functools

import jax
import jax.numpy as jnp
from jax import lax
from jax.experimental import pallas as pl
from jax.experimental.pallas import tpu as pltpu
from jax.sharding import Mesh, PartitionSpec as P


HEAD_DIM = 64
EXPERTS = 16
CAP = 8
EPSILON = 1e-06
MASKED = -1e30
EP = ("z", "x", "c")
F32 = jnp.float32
BF16 = jnp.bfloat16


def shifted(value, axis, step):
    n = lax.axis_size(axis)
    return lax.ppermute(value, axis, [(i, (i + step) % n) for i in range(n)])


def exchange(blocks, axis):
    return lax.all_to_all(blocks, axis, split_axis=0, concat_axis=0, tiled=True)


def expert_kernel(nx, rows_ref, gate_refs, up_refs, down_refs, out_ref):
    blocks, part, width = rows_ref.shape
    ny = blocks // nx
    gates, ups = [None] * len(gate_refs), [None] * len(up_refs)
    for y in range(ny):
        taken = jnp.concatenate([rows_ref[x * ny + y] for x in range(nx)], axis=0)
        deep = pl.ds(y * width, width)
        for sums, refs in ((gates, gate_refs), (ups, up_refs)):
            for k, ref in enumerate(refs):
                one = jnp.dot(taken, ref[deep, :], preferred_element_type=F32)
                sums[k] = one if sums[k] is None else sums[k] + one
    hidden = [
        (gate / (1.0 + jnp.exp(-gate)) * up).astype(BF16) for gate, up in zip(gates, ups)
    ]
    for y in range(ny):
        wide = pl.ds(y * width, width)
        back = None
        for one, ref in zip(hidden, down_refs):
            more = jnp.dot(one, ref[:, wide], preferred_element_type=F32)
            back = more if back is None else back + more
        back = back.astype(BF16)
        for x in range(nx):
            out_ref[x * ny + y] = back[x * part : (x + 1) * part]


def expert_rows(blocks, gates, ups, downs, nx):
    in_vmem = pl.BlockSpec(memory_space=pltpu.VMEM)
    count = len(gates)
    return pl.pallas_call(
        functools.partial(expert_kernel, nx),
        out_shape=jax.ShapeDtypeStruct(blocks.shape, BF16),
        in_specs=[in_vmem] + [[in_vmem] * count] * 3,
        out_specs=in_vmem,
        compiler_params=pltpu.CompilerParams(vmem_limit_bytes=20 * 2**20),
        cost_estimate=pl.CostEstimate(
            flops=2 * blocks.size * 3 * count * gates[0].shape[1],
            bytes_accessed=4 * blocks.size + 6 * count * gates[0].size,
            transcendentals=0,
        ),
    )(blocks, gates, ups, downs)


def settle_kernel(mix_refs, tokens_ref, gains_ref, selector_ref, packed_ref, cols_ref, whole_s):
    mix = None
    for ref in mix_refs:
        one = ref[...].astype(F32)
        mix = one if mix is None else mix + one
    cols = cols_ref.shape[1]
    mix = mix * lax.rsqrt(jnp.mean(mix * mix, axis=1, keepdims=True) + EPSILON)
    whole = tokens_ref[...].astype(F32) + mix * gains_ref[pl.ds(0, 1), :]
    whole_s[...] = whole
    scale = lax.rsqrt(jnp.mean(whole * whole, axis=1, keepdims=True) + EPSILON)
    here = pl.ds(pl.multiple_of(lax.axis_index("y") * cols, cols), cols)
    residual = whole_s[:, here]
    cols_ref[...] = residual
    taken = (residual * scale * gains_ref[pl.ds(1, 1), here]).astype(BF16)
    packed = jnp.dot(selector_ref[...], taken, preferred_element_type=F32)
    packed_ref[...] = packed.astype(BF16)


def settle(mixes, tokens, gains, selector, cols):
    rows, width = tokens.shape
    in_vmem = pl.BlockSpec(memory_space=pltpu.VMEM)
    return pl.pallas_call(
        settle_kernel,
        out_shape=(
            jax.ShapeDtypeStruct((selector.shape[0], cols), BF16),
            jax.ShapeDtypeStruct((rows, cols), F32),
        ),
        in_specs=[[in_vmem] * len(mixes)] + [in_vmem] * 3,
        out_specs=(in_vmem,) * 2,
        scratch_shapes=[pltpu.VMEM((rows, width), F32)],
        compiler_params=pltpu.CompilerParams(vmem_limit_bytes=6 * 2**20),
    )(mixes, tokens, gains, selector)


def fold_kernel(partials_ref, out_ref):
    nz, slots, _ = out_ref.shape
    blocks, rows, _ = partials_ref.shape
    each = rows // nz
    local_experts = slots // each
    share = blocks // local_experts
    for e in range(local_experts):
        total = partials_ref[e * share].astype(F32)
        for k in range(1, share):
            total = total + partials_ref[e * share + k].astype(F32)
        total = total.astype(BF16)
        for z in range(nz):
            out_ref[z, pl.ds(e * each, each), :] = total[z * each : (z + 1) * each]


def fold_partials(partials, local_experts, nz):
    _, rows, cols = partials.shape
    return pl.pallas_call(
        fold_kernel,
        out_shape=jax.ShapeDtypeStruct((nz, local_experts * rows // nz, cols), BF16),
        in_specs=[pl.BlockSpec(memory_space=pltpu.VMEM)],
        out_specs=pl.BlockSpec(memory_space=pltpu.VMEM),
        compiler_params=pltpu.CompilerParams(vmem_limit_bytes=6 * 2**20),
    )(partials)


def join_kernel(query_ref, key_ref, value_ref, out_ref, query_s, key_s, value_s, sems):
    parts = fetched((query_ref, key_ref, value_ref), (query_s, key_s, value_s), sems)
    joined = jnp.concatenate([part[...] for part in parts], axis=1)
    for k in range(out_ref.shape[0]):
        out_ref[k] = joined


def join(arrays, copies):
    rows = arrays[0].shape[0]
    cols = sum(array.shape[1] for array in arrays)
    return pl.pallas_call(
        join_kernel,
        out_shape=jax.ShapeDtypeStruct((copies, rows, cols), BF16),
        in_specs=[pl.BlockSpec(memory_space=pltpu.HBM)] * 3,
        out_specs=pl.BlockSpec(memory_space=pltpu.VMEM),
        scratch_shapes=places_for(arrays),
        compiler_params=pltpu.CompilerParams(vmem_limit_bytes=4 * 2**20),
    )(*in_hbm(*arrays))


def attend_kernel(
    together,
    parts,
    own_ref,
    pieces_refs,
    scale_ref,
    gate_ref,
    length_ref,
    cum_ref,
    early_keys_ref,
    keys_ref,
    values_ref,
    out_w_ref,
    mix_ref,
    key_ref,
    value_ref,
    q_s,
    own_s,
    weight_s,
    heads_s,
    past_s,
    keys_s,
    values_s,
    out_w_s,
    sems,
):
    rows, group, head_dim = q_s.shape
    span_len = keys_ref.shape[2]
    cols = group * head_dim
    scale = HEAD_DIM ** (-0.5)
    share = rows // parts
    halves = [pl.ds(p * share, share) for p in range(parts)]

    def copies(number, source, target):
        return [
            pltpu.make_async_copy(source.at[h], target.at[h], sems.at[number, p])
            for p, h in enumerate(halves)
        ]

    late = halves[1]
    key_copy = pltpu.make_async_copy(keys_ref.at[late], keys_s, sems.at[0, 0])
    out_w_copy = pltpu.make_async_copy(out_w_ref, out_w_s, sems.at[0, 1])
    value_copies = copies(1, values_ref, values_s)
    key_copy.start()
    for copy in value_copies:
        copy.start()
    out_w_copy.start()

    projected = own_ref[...]
    for ref in pieces_refs:
        projected = projected + ref[...].astype(F32)
    projected = projected * scale_ref[...]
    new_key = projected[:, cols : cols + head_dim].astype(BF16)
    new_value = projected[:, cols + head_dim : cols + 2 * head_dim].astype(BF16)
    key_ref[...] = new_key
    value_ref[...] = new_value

    query = projected[:, :cols].astype(BF16).astype(F32)
    at_head = lax.broadcasted_iota(jnp.int32, (rows, group, cols), 1)
    of_head = lax.shift_right_logical(
        lax.broadcasted_iota(jnp.int32, (rows, group, cols), 2), head_dim.bit_length() - 1
    )
    on_head = at_head == of_head
    spread = jnp.where(on_head, jnp.broadcast_to(query[:, None, :], (rows, group, cols)), 0.0)
    spread = spread.reshape(rows * group, cols).astype(BF16)
    fold = (
        lax.bitwise_and(lax.broadcasted_iota(jnp.int32, (cols, head_dim), 0), head_dim - 1)
        == lax.broadcasted_iota(jnp.int32, (cols, head_dim), 1)
    )
    fold = jnp.where(fold, 1.0, 0.0).astype(BF16)
    by_head = jnp.dot(spread, fold, preferred_element_type=F32).reshape(rows, group, head_dim)
    q_s[...] = by_head
    own_s[...] = (
        jnp.sum(by_head * new_key.astype(F32)[:, None, :], axis=2, keepdims=True) * scale
    )
    places = lax.broadcasted_iota(jnp.int32, (group, span_len), 1)

    def weigh(some):
        scores = [
            jnp.dot(
                q_s[b].astype(BF16),
                early_keys_ref[b] if b < share else keys_s[b - share],
                preferred_element_type=F32,
            )
            * scale
            for b in some
        ]
        lengths = [length_ref[b] for b in some]
        cums = [cum_ref[b] for b in some]
        lasts = [
            jnp.sum(jnp.where(places == n - 1, cum, 0.0), axis=1, keepdims=True)
            for n, cum in zip(lengths, cums)
        ]
        pasts = [
            jnp.where(places < n, score + ((last + gate_ref[b]) - cum), MASKED)
            for b, n, score, last, cum in zip(some, lengths, scores, lasts, cums)
        ]
        owns = [own_s[b] for b in some]
        peaks = [
            jnp.maximum(jnp.max(past, axis=1, keepdims=True), own)
            for past, own in zip(pasts, owns)
        ]
        past_exps = [jnp.exp(past - peak) for past, peak in zip(pasts, peaks)]
        own_exps = [jnp.exp(own - peak) for own, peak in zip(owns, peaks)]
        totals = [
            jnp.sum(past_exp, axis=1, keepdims=True) + own_exp
            for past_exp, own_exp in zip(past_exps, own_exps)
        ]
        for b, past_exp, own_exp, total in zip(some, past_exps, own_exps, totals):
            weight_s[b] = own_exp / total
            past_s[b] = (past_exp / total).astype(BF16)

    def mix(some):
        mixed = [
            lax.dot_general(
                past_s[b], values_s[b], (((1,), (1,)), ((), ())), preferred_element_type=F32
            )
            for b in some
        ]
        for b, one in zip(some, mixed):
            heads_s[b] = one

    for p in range(parts):
        if p > 0:
            key_copy.wait()
        for first in range(p * share, (p + 1) * share, together):
            weigh(range(first, first + together))
    for p in range(parts):
        value_copies[p].wait()
        mix(range(p * share, (p + 1) * share))
    own_weight = weight_s[...].astype(BF16).astype(F32)
    heads = heads_s[...] + own_weight * new_value.astype(F32)[:, None, :]
    heads = heads.reshape(rows * group, head_dim).astype(BF16)
    wide = lax.dot_general(heads, fold, (((1,), (1,)), ((), ())), preferred_element_type=F32)
    wide = jnp.where(on_head, wide.reshape(rows, group, cols), 0.0)
    heads_out = jnp.sum(wide, axis=1).astype(BF16)
    out_w_copy.wait()
    mix_ref[...] = jnp.dot(heads_out, out_w_s[...], preferred_element_type=F32).astype(BF16)


def load_kernel(count, *refs):
    sources, targets = refs[:count], refs[count:-1]
    sources = [
        source.at[pl.ds(0, target.shape[0])] for source, target in zip(sources, targets)
    ]
    fetched(sources, targets, refs[-1])


def load(arrays, heights):
    return pl.pallas_call(
        functools.partial(load_kernel, len(arrays)),
        out_shape=[
            jax.ShapeDtypeStruct((height, *array.shape[1:]), array.dtype)
            for array, height in zip(arrays, heights)
        ],
        in_specs=[pl.BlockSpec(memory_space=pltpu.HBM)] * len(arrays),
        out_specs=[pl.BlockSpec(memory_space=pltpu.VMEM)] * len(arrays),
        scratch_shapes=[pltpu.SemaphoreType.DMA((len(arrays),))],
        compiler_params=pltpu.CompilerParams(vmem_limit_bytes=8 * 2**20),
    )(*in_hbm(*arrays))


def attend(own, pieces, scale, gate, lengths, cum, early_keys, keys, values, out_w):
    rows, group, _ = cum.shape
    head_dim, width = keys.shape[1], out_w.shape[1]
    in_vmem = pl.BlockSpec(memory_space=pltpu.VMEM)
    from_hbm = pl.BlockSpec(memory_space=pltpu.HBM)
    one = jax.ShapeDtypeStruct((rows, head_dim), BF16)
    together, parts = 8, 2
    return pl.pallas_call(
        functools.partial(attend_kernel, together, parts),
        out_shape=(jax.ShapeDtypeStruct((rows, width), BF16), one, one),
        in_specs=[in_vmem, [in_vmem] * len(pieces)]
        + [in_vmem] * 5
        + [from_hbm] * 3,
        out_specs=(in_vmem,) * 3,
        scratch_shapes=[
            pltpu.VMEM((rows, group, head_dim), F32),
            pltpu.VMEM((rows, group, 1), F32),
            pltpu.VMEM((rows, group, 1), F32),
            pltpu.VMEM((rows, group, head_dim), F32),
            pltpu.VMEM(cum.shape, BF16),
            pltpu.VMEM((rows // parts, *keys.shape[1:]), BF16),
            pltpu.VMEM(values.shape, BF16),
            pltpu.VMEM(out_w.shape, BF16),
            pltpu.SemaphoreType.DMA((2, parts)),
        ],
        compiler_params=pltpu.CompilerParams(vmem_limit_bytes=24 * 2**20),
        cost_estimate=pl.CostEstimate(
            flops=4 * keys.size * group + 2 * rows * out_w.size,
            bytes_accessed=4 * keys.size + 4 * cum.size + 2 * out_w.size,
            transcendentals=cum.size,
        ),
    )(own, pieces, scale, gate, lengths, cum, early_keys, *in_hbm(keys, values, out_w))


def cut_kernel(nz, nx, *refs):
    outs, cut_s = refs[2 : 2 + nx], refs[2 + nx]
    tokens_ref, gain_ref = fetched(refs[:2], refs[3 + nx : -1], refs[-1])
    _, width = tokens_ref.shape
    chunk = width // (nz * nx)
    scaled = (tokens_ref[...].astype(F32) * gain_ref[...])
    for x in range(nx):
        cut_s[x] = jnp.concatenate(
            [scaled[:, (z * nx + x) * chunk : (z * nx + x + 1) * chunk] for z in range(nz)], axis=1
        )
    here = lax.axis_index("x")
    for s in range(nx):
        outs[s][...] = cut_s[lax.rem(here + s, nx)].astype(BF16)


def cut_tokens(tokens, gain, nz, nx):
    rows, width = tokens.shape
    in_vmem = pl.BlockSpec(memory_space=pltpu.VMEM)
    return pl.pallas_call(
        functools.partial(cut_kernel, nz, nx),
        out_shape=[jax.ShapeDtypeStruct((rows, width // nx), BF16)] * nx,
        in_specs=[pl.BlockSpec(memory_space=pltpu.HBM)] * 2,
        out_specs=[in_vmem] * nx,
        scratch_shapes=[pltpu.VMEM((nx, rows, width // nx), F32)] + places_for((tokens, gain)),
        compiler_params=pltpu.CompilerParams(vmem_limit_bytes=4 * 2**20),
    )(*in_hbm(tokens, gain))


def multiply_kernel(count, *refs):
    token_refs, (same_ref, other_ref), outs = refs[:count], refs[count : count + 2], refs[count + 2 :]
    first = lax.axis_index("c") == 0
    same, other = same_ref[...], other_ref[...]
    weights = jnp.concatenate(
        (jnp.where(first, same, other), jnp.where(first, other, same)), axis=1
    )
    weights = weights.reshape(-1, weights.shape[-1])
    tokens = jnp.concatenate([ref[...] for ref in token_refs], axis=0)
    product = jnp.dot(tokens, weights, preferred_element_type=F32)
    rows = token_refs[0].shape[0]
    for s, out in enumerate(outs):
        out[...] = product[s * rows : (s + 1) * rows].astype(out.dtype)


def multiply(pieces, same, other):
    rows = pieces[0].shape[0]
    cols = same.shape[2]
    in_vmem = pl.BlockSpec(memory_space=pltpu.VMEM)
    kinds = [F32] + [BF16] * (len(pieces) - 1)
    return pl.pallas_call(
        functools.partial(multiply_kernel, len(pieces)),
        out_shape=[jax.ShapeDtypeStruct((rows, cols), kind) for kind in kinds],
        in_specs=[in_vmem] * (len(pieces) + 2),
        out_specs=[in_vmem] * len(pieces),
        compiler_params=pltpu.CompilerParams(vmem_limit_bytes=8 * 2**20),
        cost_estimate=pl.CostEstimate(
            flops=4 * rows * len(pieces) * same.size,
            bytes_accessed=4 * same.size,
            transcendentals=0,
        ),
    )(*pieces, same, other)


def fetched(sources, targets, sems):
    copies = [
        pltpu.make_async_copy(source, target, sems.at[k])
        for k, (source, target) in enumerate(zip(sources, targets))
    ]
    for copy in copies:
        copy.start()
    for copy in copies:
        copy.wait()
    return targets


def in_hbm(*arrays):
    return [pltpu.with_memory_space_constraint(array, pltpu.HBM) for array in arrays]


def places_for(arrays):
    return [pltpu.VMEM(array.shape, array.dtype) for array in arrays] + [
        pltpu.SemaphoreType.DMA((len(arrays),))
    ]


def early_kernel(count, *refs):
    (
        scale_ref,
        log_gate_ref,
        gate_ref,
        long_ref,
        selector_ref,
        weighing_ref,
        kept_ref,
        gains_ref,
    ) = refs[count : count + 8]
    (
        tokens_ref,
        gain_ref,
        gain_mix_ref,
        gain_ffn_ref,
        forget_ref,
        bias_ref,
        length_ref,
        routes_ref,
        weights_ref,
    ) = fetched(refs[:count], refs[count + 8 : -1], refs[-1])
    kept_ref[...] = tokens_ref[...]
    gains_ref[pl.ds(0, 1), :] = gain_mix_ref[...]
    gains_ref[pl.ds(1, 1), :] = gain_ffn_ref[...]

    tokens = tokens_ref[...].astype(F32)
    rows = tokens.shape[0]
    group = forget_ref.shape[0]
    scale = lax.rsqrt(jnp.mean(tokens * tokens, axis=1, keepdims=True) + EPSILON)
    scale_ref[...] = scale
    normed = (tokens * scale * gain_ref[...]).astype(BF16)
    logits = lax.dot_general(
        normed, forget_ref[...], (((1,), (1,)), ((), ())), preferred_element_type=F32
    )
    logits = logits + bias_ref[...]
    gate = jnp.minimum(logits, 0.0) - jnp.log1p(jnp.exp(-jnp.abs(logits)))
    across = lax.dot_general(
        forget_ref[...], normed, (((1,), (1,)), ((), ())), preferred_element_type=F32
    )
    one = lax.broadcasted_iota(jnp.int32, (group, group), 0) == lax.broadcasted_iota(
        jnp.int32, (group, group), 1
    )
    across = across + jnp.sum(jnp.where(one, bias_ref[...], 0.0), axis=1, keepdims=True)
    log_gate_ref[...] = jnp.minimum(across, 0.0) - jnp.log1p(jnp.exp(-jnp.abs(across)))
    same = lax.broadcasted_iota(jnp.int32, (rows, group, group), 1) == lax.broadcasted_iota(
        jnp.int32, (rows, group, group), 2
    )
    gate_ref[...] = jnp.sum(jnp.where(same, gate[:, None, :], 0.0), axis=2, keepdims=True)
    mine = lax.broadcasted_iota(jnp.int32, (rows, rows), 0) == lax.broadcasted_iota(
        jnp.int32, (rows, rows), 1
    )
    lengths = jnp.where(mine, length_ref[...].astype(F32), 0.0)
    lengths = jnp.sum(lengths, axis=1, keepdims=True)
    long_ref[...] = jnp.broadcast_to(lengths[:, None, :], long_ref.shape).astype(jnp.int32)

    top = routes_ref.shape[0]
    named = [routes_ref[pl.ds(k, 1), :] for k in range(top)]
    experts = lax.broadcasted_iota(jnp.int32, (EXPERTS, rows), 0)
    hits = [jnp.where(experts == one, 1.0, 0.0) for one in named]
    both = sum(hits[1:], hits[0])
    before = lax.broadcasted_iota(jnp.int32, (rows, rows), 0) < lax.broadcasted_iota(
        jnp.int32, (rows, rows), 1
    )
    earlier = jnp.dot(
        both.astype(BF16), jnp.where(before, 1.0, 0.0).astype(BF16), preferred_element_type=F32
    )
    places = lax.broadcasted_iota(jnp.int32, (EXPERTS * CAP, rows), 0)
    chosen = jnp.zeros((EXPERTS * CAP, rows), F32)
    weighed = jnp.zeros((EXPERTS * CAP, rows), F32)
    for k in range(top):
        slot = jnp.sum(earlier * hits[k], axis=0, keepdims=True).astype(jnp.int32)
        there = jnp.where(places == named[k] * CAP + slot, 1.0, 0.0)
        chosen = chosen + there
        weighed = weighed + there * weights_ref[pl.ds(k, 1), :]
    selector_ref[...] = chosen.astype(BF16)
    weighing_ref[...] = weighed


def early(*arrays):
    in_vmem = pl.BlockSpec(memory_space=pltpu.VMEM)
    tokens, _, _, _, forget, *_ = arrays
    rows, group = tokens.shape[0], forget.shape[0]
    slots = EXPERTS * CAP
    return pl.pallas_call(
        functools.partial(early_kernel, len(arrays)),
        out_shape=(
            jax.ShapeDtypeStruct((rows, 1), F32),
            jax.ShapeDtypeStruct((group, rows), F32),
            jax.ShapeDtypeStruct((rows, group, 1), F32),
            jax.ShapeDtypeStruct((rows, group, 1), jnp.int32),
            jax.ShapeDtypeStruct((slots, rows), BF16),
            jax.ShapeDtypeStruct((slots, rows), F32),
            jax.ShapeDtypeStruct(tokens.shape, BF16),
            jax.ShapeDtypeStruct((2, tokens.shape[1]), F32),
        ),
        in_specs=[pl.BlockSpec(memory_space=pltpu.HBM)] * len(arrays),
        out_specs=(in_vmem,) * 8,
        scratch_shapes=places_for(arrays),
        compiler_params=pltpu.CompilerParams(vmem_limit_bytes=6 * 2**20),
    )(*in_hbm(*arrays))


def layer(
    tokens,
    norm_gain_attn,
    w_query,
    w_key,
    w_value,
    w_forget,
    forget_bias,
    cache_keys,
    cache_values,
    cache_logcum,
    lengths,
    w_out,
    norm_gain_mix,
    norm_gain_ffn,
    expert_gate,
    expert_up,
    expert_down,
    routes,
    route_weights,
):
    rows, width = tokens.shape
    nz, nx, _, ny = (lax.axis_size(a) for a in ("z", "x", "c", "y"))

    scale_attn, new_log_gate, gate, long, selector, weighing, kept, gains = early(
        tokens,
        norm_gain_attn.reshape(1, width),
        norm_gain_mix.reshape(1, width),
        norm_gain_ffn.reshape(1, width),
        w_forget.T,
        forget_bias.reshape(1, -1),
        lengths.reshape(1, -1),
        routes.T,
        route_weights.T,
    )

    weights = join((w_query, w_key, w_value), nz)
    same_core = exchange(weights, "z")
    others = [shifted(w, "c", 1) for w in (expert_gate, expert_up, expert_down)]
    other_core = shifted(same_core, "c", 1)
    mine = cut_tokens(tokens, norm_gain_attn.reshape(1, width), nz, nx)
    moved = [shifted(mine[s], "x", s) for s in range(1, nx)]
    own_partial, *partials = multiply([mine[0]] + moved, same_core, other_core)
    pieces = [shifted(partials[s - 1], "x", nx - s) for s in range(1, nx)]

    logcum, early_keys = load((cache_logcum, cache_keys), (rows, rows // 2))

    partial_mix, new_keys, new_values = attend(
        own_partial,
        pieces,
        scale_attn,
        gate,
        long,
        logcum,
        early_keys,
        cache_keys,
        cache_values,
        w_out,
    )

    mixes = [partial_mix] + [shifted(partial_mix, "y", s) for s in range(1, ny)]
    col_width = width // ny
    packed, residual_cols = settle(mixes, kept, gains, selector, col_width)

    local_experts = EXPERTS // nz
    spread = nx // local_experts
    on_z = exchange(packed.reshape(nz, local_experts * CAP, col_width), "z")
    on_z = on_z.reshape(nz, local_experts, CAP, col_width).transpose(1, 0, 2, 3)
    on_z = on_z.reshape(local_experts, 1, 1, nz * CAP, col_width)
    outgoing = jnp.broadcast_to(on_z, (local_experts, spread, ny, nz * CAP, col_width))
    own = exchange(outgoing.reshape(nx * ny, nz * CAP, col_width), ("x", "y"))
    part = expert_rows(own, *[list(p) for p in zip((expert_gate, expert_up, expert_down), others)], nx)
    summed = exchange(part, ("x", "y"))
    returned = exchange(fold_partials(summed, local_experts, nz), "z")
    returned = returned.reshape(EXPERTS * CAP, col_width)
    routed = lax.dot_general(
        weighing, returned.astype(F32), (((0,), (0,)), ((), ())), preferred_element_type=F32
    )
    layer_out = (residual_cols + routed).astype(BF16)
    return (layer_out, new_keys, new_values, new_log_gate.T)


def solution(mesh):
    chips = Mesh(mesh.devices.reshape(8, 4, 2, 4), ("z", "x", "c", "y"))
    everyone = ("z", "x", "c", "y")
    placed = (
        P(EP, None),
        P(),
        P(EP, "y"),
        P(EP, "y"),
        P(EP, "y"),
        P(None, "y"),
        P("y"),
        P(EP, "y", None),
        P(EP, "y", None),
        P(EP, "y", None),
        P(EP),
        P("y", None),
        P(),
        P(),
        P(None, everyone),
        P(None, everyone),
        P(everyone, None),
        P(EP, None),
        P(EP, None),
    )
    return jax.shard_map(
        layer,
        mesh=chips,
        in_specs=placed,
        out_specs=(P(EP, "y"), P(EP, "y"), P(EP, "y"), P(EP, "y")),
        check_vma=False,
    )
```
